32 devices in a mesh: grp: 2 (over x), ep: 4 (over y, core), tp: 4 (over z).
Axes of the slice: x: 2, y: 2, z: 4, core: 2. Of those that a mesh axis runs over, the one named last changes fastest.
Arguments:
- tokens: bfloat16 [4096, 1024], P(('grp', 'ep', 'tp')), parts along dimension 0, may hold values from -6 to 6
- norm_gain: float32 [1024], replicated, may hold values from 0.1 to 1.9
- gate_weight: bfloat16 [4, 1024, 3584], P('ep', None, 'tp'), may hold values from -0.1875 to 0.1875
- up_weight: bfloat16 [4, 1024, 3584], P('ep', None, 'tp'), may hold values from -0.1875 to 0.1875
- down_weight: bfloat16 [4, 3584, 1024], P('ep', 'tp'), may hold values from -0.09375 to 0.09375
- expert_ids: int32 [4096, 2], P(('grp', 'ep')), parts along dimension 0, may hold values from 0 to 3, all different within a row; in each aligned block of 128 rows (0 to 127, 128 to 255, ...) at most 80 rows name the same one
- route_weight: float32 [4096, 2], P(('grp', 'ep')), parts along dimension 0, may hold values from 0.2 to 1
Outputs:
- mixed: bfloat16 [4096, 1024], P(('grp', 'ep', 'tp')), parts along dimension 0
The draws below stay inside these ranges and needn't reach their ends.
There are 2 independent parts, one for each index of `grp`. The reference program is written for one: setup_inputs(seed, part) draws one part's arguments, and reference() takes and returns one part's arrays. A program takes and returns all parts, laid end to end along the dimension named above; an argument that names none is the same for every part. Nothing has to cross between parts.
Inputs may be any that keep to these rules, and one draw needn't show every extreme that they name: `expert_ids`: A token's 2 experts differ. In the rows of one device (128 tokens, aligned blocks) no expert is named more than 80 times, and in every draw some expert is named exactly 80 times in some device's rows.
All inputs are finite; a program needn't handle non-finite values.
Results may differ from the reference program's by a relative error of at most 0.015.
Values may be sent and summed in bfloat16 or wider, within the bound.
A program may use at most 64 MiB of HBM per device.

```python
import math
import jax
import jax.numpy as jnp
import numpy as np
from jax import lax

D = 1024
FF = 3584
TOP_K = 2
TOK_DEV = 128
EXPERTS = 4
TOKENS = 2048
MOST = 80
N_EP = 4
N_TP = 4


def shard_levels(rng, shape, split, least, high):
    gain = 1.0
    for position, shards_of in split:
        steps = jax.random.uniform(jax.random.fold_in(jax.random.fold_in(rng, 6), position), (shards_of,), jnp.float32, least / len(split), high / len(split))
        gain = gain * jnp.repeat(jnp.exp(steps), shape[position] // shards_of).reshape((-1,) + (1,) * (len(shape) - 1 - position))
    return gain


def deal_out(rng, own, number, rows, count, top, most, skew):
    sequence = jax.random.permutation(rng, count)
    crowded, usual = portions_of(count, rows * top, most, skew, True), portions_of(count, rows * top, most, skew, False)
    places = jnp.arange(count)

    def named(lengths, turn):
        used = int((lengths > 0).sum())
        fixed = max(1, used // 4)
        moved = fixed + (places - fixed + turn * (used - fixed)) % max(1, count - fixed)
        return jnp.zeros((count,), jnp.int32).at[sequence[jnp.where(places < fixed, places, moved)]].set(jnp.asarray(lengths, jnp.int32))

    lengths = jnp.where(number % 4 == 0, named(crowded, number // 4), named(usual, number - number // 4 - 1))
    mixed = jax.random.permutation(jax.random.fold_in(own, 3), count)
    giver, sink = mixed[0:count // 2 * 2:2], mixed[1:count // 2 * 2:2]
    slack = jnp.minimum(lengths[giver] - 1, most - lengths[sink]) // 2
    slack = jnp.where((giver == sequence[0]) | (sink == sequence[0]) | (lengths[sink] == 0), 0, jnp.maximum(slack, 0))
    moved = jax.random.randint(jax.random.fold_in(own, 4), (count // 2,), 0, 1 << 20) % (slack + 1)
    lengths = lengths.at[giver].add(-moved).at[sink].add(moved)
    items = jnp.searchsorted(jnp.cumsum(lengths), jnp.arange(rows * top), side="right").astype(jnp.int32)
    table = items.reshape(top, rows).T
    table = table[jax.random.permutation(jax.random.fold_in(own, 1), rows)]
    turn = jax.random.randint(jax.random.fold_in(own, 2), (rows, 1), 0, top)
    return jnp.take_along_axis(table, (jnp.arange(top)[None, :] + turn) % top, axis=1)


def portions_of(count, total, most, lean, full):
    weights = [(1 << 20) // math.isqrt(grade ** lean) + 1 for grade in range(1, count + 1)]
    largest = most if full else min(most, max(-(-total // count), total * weights[0] // sum(weights)))
    least = 1 if total - largest >= count - 1 else 0
    given, rest = [largest] + [least] * (count - 1), total - largest - least * (count - 1)
    while rest > 0:
        candidates = [i for i in range(1, count) if given[i] < largest] or [i for i in range(1, count) if given[i] < most]
        pool, budget = sum([weights[i] for i in candidates]), rest
        for i in candidates:
            more = min(most - given[i], max(1, budget * weights[i] // pool), rest)
            given[i] = given[i] + more
            rest = rest - more
    return np.array(given)


def centred(rng, extent, spread, bound, shards=(), held_as=jnp.bfloat16):
    result = jax.random.normal(rng, extent, jnp.float32) * spread
    if len(shards) > 0:
        result = shard_levels(rng, extent, shards, -0.22, 0.18) * result
    return jnp.clip(result, min=-bound, max=bound).astype(held_as)


def setup_inputs(seed: int = 0, part: int = 0) -> dict:
    streams_of = jax.random.split(jax.random.key(seed), 8)
    own_keys = jax.random.split(jax.random.fold_in(streams_of[7], part), 8)
    tokens = centred(own_keys[0], (TOKENS, D), 1.0, 6.0, ((0, 16),))
    norm_gain = jnp.clip(1.0 + 0.18 * jax.random.normal(streams_of[1], (D,), jnp.float32), 0.1, 1.9)
    gate_weight = centred(streams_of[2], (EXPERTS, D, FF), D ** -0.5, 0.1875, ((0, 4), (2, 4)))
    up_weight = centred(streams_of[3], (EXPERTS, D, FF), D ** -0.5, 0.1875, ((0, 4), (2, 4)))
    down_weight = centred(streams_of[4], (EXPERTS, FF, D), FF ** -0.5, 0.09375, ((0, 4), (1, 4)))
    expert_ids_keys = jax.random.split(jax.random.fold_in(own_keys[5], 1), TOKENS // TOK_DEV)
    expert_ids_turns = jax.random.permutation(jax.random.fold_in(own_keys[5], 3), TOKENS // TOK_DEV)
    expert_ids = jax.vmap(lambda own, number: deal_out(jax.random.fold_in(own_keys[5], 2), own, number, TOK_DEV, EXPERTS, TOP_K, MOST, 2))(expert_ids_keys, expert_ids_turns).reshape((TOKENS, TOP_K))
    route_weight = jnp.clip(0.2 + 0.8 * jax.random.uniform(own_keys[6], (TOKENS, TOP_K), jnp.float32) ** shard_levels(own_keys[6], (TOKENS, TOP_K), ((0, 4),), -0.2, 0.2), 0.2, 1.0)
    return dict(tokens=tokens, norm_gain=norm_gain, gate_weight=gate_weight, up_weight=up_weight, down_weight=down_weight, expert_ids=expert_ids, route_weight=route_weight)


def norm_rows(tokens, norm_gain):
    values = tokens.astype(jnp.float32)
    scaled = values * lax.rsqrt(lax.optimization_barrier(jnp.mean(values * values, axis=-1, keepdims=True)) + 1e-06)
    return (scaled * norm_gain.astype(jnp.float32)).astype(jnp.bfloat16)

def reference(tokens, norm_gain, gate_weight, up_weight, down_weight, expert_ids, route_weight):
    normed = norm_rows(tokens, norm_gain)
    devices_all = N_EP * N_TP
    cap_rows = devices_all * MOST
    flat_ids = expert_ids.astype(jnp.int32).reshape(devices_all, TOK_DEV * TOP_K)
    onehot = (flat_ids[:, :, None] == jnp.arange(EXPERTS, dtype=jnp.int32)[None, None, :]).astype(jnp.int32)
    before = jnp.cumsum(onehot, axis=1) - onehot
    slots = lax.optimization_barrier(jnp.sum(before * onehot, axis=-1))
    owner = jnp.arange(devices_all, dtype=jnp.int32)[:, None]
    row_index = (flat_ids * cap_rows + owner * MOST + slots).reshape(-1).astype(jnp.int32)
    repeated = jnp.repeat(normed, TOP_K, axis=0)
    buffer = jnp.zeros((EXPERTS * cap_rows, D), jnp.bfloat16).at[row_index].set(repeated)
    buffer = buffer.reshape(EXPERTS, cap_rows, D)
    block = FF // N_TP

    def shard_step(total, shard):
        start = (shard * block).astype(jnp.int32)

        def one_expert(items):
            rows, w_gate, w_up, w_down = items
            gate_part = lax.dynamic_slice_in_dim(w_gate, start, block, 1)
            up_part = lax.dynamic_slice_in_dim(w_up, start, block, 1)
            down_part = lax.dynamic_slice_in_dim(w_down, start, block, 0)
            gate = jnp.dot(rows, gate_part, preferred_element_type=jnp.float32)
            upper = jnp.dot(rows, up_part, preferred_element_type=jnp.float32)
            hidden = (jax.nn.silu(gate) * upper).astype(jnp.bfloat16)
            return jnp.dot(hidden, down_part, preferred_element_type=jnp.float32).astype(jnp.bfloat16)
        pieces = lax.map(one_expert, (buffer, gate_weight, up_weight, down_weight))
        picked = pieces.reshape(EXPERTS * cap_rows, D)[row_index].reshape(TOKENS, TOP_K, D)
        return (total + picked.astype(jnp.float32), None)
    total, _ = lax.scan(shard_step, jnp.zeros((TOKENS, TOP_K, D), jnp.float32), jnp.arange(N_TP, dtype=jnp.int32))
    piece = lax.optimization_barrier(total.astype(jnp.bfloat16))
    weighted = lax.optimization_barrier(jnp.sum(piece.astype(jnp.float32) * route_weight.astype(jnp.float32)[:, :, None], axis=1))
    return weighted.astype(jnp.bfloat16)
```

```python
import functools

import jax
import jax.numpy as jnp
from jax import lax
from jax.experimental import pallas as pl
from jax.experimental.pallas import tpu as pltpu
from jax.sharding import PartitionSpec as P

TOP_K = 2
MESH = pl.DeviceIdType.MESH
VMEM_ROOM = 60 << 20

ACROSS, INWARD, OUTWARD = range(3)
RELAY, SEND, REDUCE, COMPUTE = range(4)
UNITS = 2
PIECES = 4
LINE = 4
CROSSES = ((True, True, False, False), (True, True, True, False))
ORDER = (
    (
        (0, 0, 0, 0, 0), (0, 0, 0, 1, 0), (0, 0, 0, 2, 0), (0, 0, 0, 3, 0), (1, 0, 0, 1, 1), (1, 0, 0, 0, 0),
        (1, 0, 0, 2, 1), (1, 0, 0, 1, 0), (3, 0, 0, 1, 0), (1, 0, 0, 0, 1), (1, 0, 0, 2, 0), (3, 0, 0, 0, 0),
        (0, 0, 1, 2, 0), (0, 1, 0, 0, 0), (1, 0, 0, 3, 1), (1, 0, 0, 3, 0), (1, 0, 1, 2, 0), (0, 1, 0, 1, 0),
        (0, 0, 1, 1, 0), (3, 1, 0, 0, 0), (0, 1, 0, 2, 0), (0, 0, 1, 3, 0), (1, 0, 1, 1, 0), (1, 1, 0, 2, 1),
        (0, 1, 0, 3, 0), (0, 0, 2, 1, 0), (1, 0, 2, 1, 0), (1, 1, 0, 3, 1), (3, 0, 1, 1, 0), (0, 1, 1, 2, 0),
        (0, 1, 1, 3, 0), (2, 1, 0, 1, 0), (3, 1, 0, 1, 0), (0, 0, 2, 2, 0), (0, 1, 1, 1, 0), (1, 0, 2, 2, 0),
        (2, 0, 1, 3, 1), (3, 1, 1, 1, 0), (0, 1, 2, 1, 0), (0, 1, 2, 3, 0), (2, 1, 0, 0, 0), (2, 1, 1, 2, 0),
        (2, 1, 1, 3, 1), (0, 0, 3, 1, 0), (1, 0, 3, 1, 0), (0, 1, 2, 2, 0), (0, 0, 3, 2, 0), (3, 1, 2, 1, 0),
        (0, 0, 3, 3, 0), (2, 0, 1, 2, 1), (0, 0, 3, 0, 0), (1, 0, 3, 0, 0), (3, 0, 3, 1, 0), (0, 1, 3, 1, 0),
        (0, 1, 3, 2, 0), (2, 1, 2, 2, 0), (2, 1, 2, 3, 1), (3, 0, 3, 0, 0), (0, 1, 3, 3, 0), (2, 0, 3, 2, 1),
        (0, 1, 3, 0, 0), (2, 0, 3, 3, 1), (3, 1, 3, 1, 0), (0, 0, 2, 0, 0), (1, 0, 2, 0, 0), (3, 1, 3, 0, 0),
        (0, 0, 2, 3, 0), (3, 0, 2, 0, 0), (0, 0, 1, 0, 0), (2, 1, 3, 2, 1), (2, 1, 3, 1, 0), (3, 0, 2, 1, 0),
        (0, 1, 2, 0, 0), (2, 1, 3, 3, 1), (1, 0, 1, 0, 0), (3, 0, 1, 0, 0), (2, 0, 2, 2, 1), (2, 1, 3, 0, 0),
        (3, 1, 2, 0, 0), (2, 0, 3, 1, 1), (2, 0, 2, 3, 1), (0, 1, 1, 0, 0), (2, 1, 2, 0, 0), (2, 1, 2, 1, 0),
        (3, 1, 1, 0, 0), (2, 0, 3, 0, 1), (2, 1, 1, 0, 0), (2, 0, 2, 0, 1), (2, 1, 1, 1, 0), (2, 0, 2, 1, 1),
        (2, 1, 0, 2, 0), (2, 1, 0, 3, 0), (2, 0, 1, 0, 1), (2, 0, 1, 1, 1), (2, 0, 0, 1, 0), (2, 0, 0, 2, 0),
        (2, 0, 0, 3, 0), (2, 0, 0, 0, 0),
    ),
    (
        (0, 0, 1, 0, 0), (0, 0, 1, 1, 0), (0, 0, 1, 2, 0), (0, 0, 1, 3, 0), (1, 0, 1, 1, 1), (1, 0, 1, 3, 0),
        (1, 0, 1, 2, 2), (1, 0, 1, 2, 1), (1, 0, 1, 0, 0), (1, 0, 1, 1, 2), (3, 0, 1, 1, 0), (1, 0, 1, 3, 1),
        (1, 0, 1, 2, 0), (1, 0, 1, 3, 2), (3, 0, 1, 0, 0), (0, 0, 0, 1, 0), (0, 0, 2, 1, 0), (0, 1, 1, 3, 0),
        (1, 1, 1, 3, 1), (1, 0, 2, 1, 2), (1, 0, 2, 1, 0), (1, 0, 0, 1, 1), (1, 0, 1, 1, 0), (1, 1, 1, 3, 2),
        (0, 0, 0, 2, 0), (0, 0, 2, 2, 0), (0, 1, 1, 0, 0), (1, 0, 0, 2, 1), (1, 0, 2, 2, 0), (1, 0, 2, 2, 2),
        (0, 0, 0, 0, 0), (0, 0, 2, 3, 0), (0, 1, 1, 2, 0), (3, 0, 0, 0, 0), (0, 0, 0, 3, 0), (0, 1, 2, 3, 0),
        (0, 1, 2, 1, 0), (1, 0, 0, 3, 1), (1, 0, 0, 0, 0), (1, 1, 2, 3, 2), (3, 1, 1, 1, 0), (0, 0, 3, 1, 0),
        (0, 1, 1, 1, 0), (1, 0, 0, 0, 1), (1, 0, 3, 1, 2), (1, 0, 3, 1, 0), (3, 0, 0, 1, 0), (0, 1, 0, 2, 0),
        (0, 0, 3, 2, 0), (0, 1, 2, 2, 0), (1, 1, 0, 2, 1), (2, 1, 1, 2, 0), (1, 0, 3, 2, 2), (3, 1, 1, 0, 0),
        (0, 1, 0, 3, 0), (0, 0, 3, 3, 0), (0, 1, 0, 0, 0), (1, 1, 0, 3, 1), (1, 0, 3, 3, 2), (1, 0, 0, 1, 0),
        (3, 0, 2, 1, 0), (0, 0, 3, 0, 0), (0, 1, 3, 1, 0), (2, 1, 1, 0, 0), (1, 0, 1, 0, 1), (1, 0, 3, 0, 2),
        (3, 0, 3, 1, 0), (0, 1, 3, 2, 0), (1, 1, 3, 2, 2), (1, 0, 3, 0, 0), (3, 0, 3, 0, 0), (0, 1, 3, 3, 0),
        (0, 1, 0, 1, 0), (1, 1, 3, 3, 2), (2, 1, 1, 1, 0), (3, 1, 2, 1, 0), (0, 0, 2, 0, 0), (1, 0, 2, 0, 0),
        (1, 0, 2, 0, 2), (3, 1, 0, 1, 0), (3, 0, 2, 0, 0), (0, 1, 3, 0, 0), (2, 1, 2, 2, 0), (1, 0, 2, 3, 2),
        (3, 1, 0, 0, 0), (1, 0, 1, 0, 2), (3, 1, 3, 0, 0), (0, 1, 2, 0, 0), (3, 1, 3, 1, 0), (2, 1, 2, 3, 1),
        (2, 1, 3, 0, 0), (3, 1, 2, 0, 0), (2, 0, 3, 2, 1), (2, 1, 3, 1, 0), (2, 1, 0, 0, 0), (2, 0, 3, 3, 1),
        (2, 1, 0, 1, 0), (2, 1, 2, 1, 0), (2, 0, 0, 2, 2), (2, 1, 3, 2, 1), (2, 1, 1, 3, 0), (2, 0, 0, 3, 2),
        (2, 1, 3, 3, 1), (2, 1, 2, 0, 0), (2, 0, 2, 2, 1), (2, 1, 0, 2, 2), (2, 0, 3, 1, 1), (2, 1, 0, 3, 2),
        (2, 0, 2, 3, 1), (2, 0, 1, 2, 0), (2, 0, 3, 0, 1), (2, 0, 0, 1, 2), (2, 0, 2, 0, 1), (2, 0, 1, 3, 0),
        (2, 0, 2, 1, 1), (2, 0, 0, 0, 2), (2, 0, 1, 0, 0), (2, 0, 1, 1, 0),
    ),
)


def norm_rows(tokens, norm_gain):
    values = tokens.astype(jnp.float32)
    scaled = values * lax.rsqrt(jnp.mean(values * values, axis=-1, keepdims=True) + 1e-06)
    return (scaled * norm_gain).astype(jnp.bfloat16)


def expert_hidden(rows, gate_weight, up_weight):
    gate = jnp.einsum("e...d,edf->e...f", rows, gate_weight, preferred_element_type=jnp.float32)
    upper = jnp.einsum("e...d,edf->e...f", rows, up_weight, preferred_element_type=jnp.float32)
    return (jax.nn.silu(gate) * upper).astype(jnp.bfloat16)


def weigh_pieces(summed, weights):
    piece = lax.optimization_barrier(summed.astype(jnp.bfloat16)).astype(jnp.float32)
    total = piece[:, 0] * weights[:, 0:1]
    total = total + piece[:, 1] * weights[:, 1:2]
    return total.astype(jnp.bfloat16)


def plain_body(tokens, norm_gain, gate_weight, up_weight, down_weight, expert_ids, route_weight):
    tok_rows = tokens.shape[0]
    width = tokens.shape[1]
    local_experts = gate_weight.shape[0]
    inner = gate_weight.shape[2]
    n_tp = lax.axis_size("tp")
    n_ep = lax.axis_size("ep")
    experts = n_ep * local_experts
    most = max(2, tok_rows * TOP_K * 5 // (4 * experts))
    normed = norm_rows(tokens, norm_gain)
    flat_ids = expert_ids.reshape(n_tp, tok_rows * TOP_K)
    onehot = (flat_ids[:, :, None] == jnp.arange(experts, dtype=jnp.int32)[None, None, :]).astype(
        jnp.int32
    )
    before = jnp.cumsum(onehot, axis=1) - onehot
    slots = jnp.sum(before * onehot, axis=-1)
    owner = jnp.arange(n_tp, dtype=jnp.int32)[:, None]
    row_index = (flat_ids * (n_tp * most) + owner * most + slots).reshape(-1)
    mine = lax.axis_index("tp")
    own_ids = lax.dynamic_slice_in_dim(flat_ids, mine, 1, 0)[0]
    own_slots = lax.dynamic_slice_in_dim(slots, mine, 1, 0)[0]
    own_index = own_ids * most + own_slots
    whole = lax.all_gather(normed, "tp", axis=0, tiled=True)
    sending = (
        jnp.zeros((experts * n_tp * most, width), jnp.bfloat16)
        .at[row_index]
        .set(jnp.repeat(whole, TOP_K, axis=0))
    )
    arrived = lax.all_to_all(
        sending.reshape(experts, n_tp * most, width), "ep", split_axis=0, concat_axis=1, tiled=True
    )
    hidden = expert_hidden(arrived, gate_weight, up_weight)
    by_source = hidden.reshape(local_experts, n_ep, n_tp, most, inner).transpose(2, 0, 1, 3, 4)
    per_device = local_experts * n_ep * most
    product = jnp.einsum(
        "tlnmf,lfd->tlnmd", by_source, down_weight, preferred_element_type=jnp.float32
    )
    own_sums = lax.psum_scatter(
        product.astype(jnp.bfloat16)
        .astype(jnp.float32)
        .reshape(per_device * lax.axis_size("tp"), width)
        .astype(jnp.bfloat16),
        "tp",
        scatter_dimension=0,
        tiled=True,
    )
    own_pieces = own_sums.reshape(local_experts, n_ep, most, width)
    back = lax.all_to_all(own_pieces, "ep", split_axis=1, concat_axis=0, tiled=True)
    picked = back.reshape(experts * most, width)[own_index].reshape(tok_rows, TOP_K, width)
    own_weights = lax.dynamic_slice_in_dim(route_weight, mine * tok_rows, tok_rows, 0)
    return weigh_pieces(picked.astype(jnp.float32), own_weights)


def neighbour(n, place, edge, piece):
    row, at, number = piece
    if edge == ACROSS:
        return place, (1 - row, at, number), ACROSS
    if edge == OUTWARD:
        return (place - 1, piece, INWARD) if place else None
    if place + 1 < n // 2:
        return place + 1, piece, OUTWARD
    return place, (row, n - 1 - at, number), INWARD


def parent(n, place, piece):
    row, at, number = piece
    if at == place:
        return ACROSS if row else None
    if row and CROSSES[min(at, n - 1 - at)][number]:
        return ACROSS
    return INWARD if at > place else OUTWARD


def children(n, place, piece):
    found = []
    for edge in (ACROSS, INWARD, OUTWARD):
        there = neighbour(n, place, edge, piece)
        if there is not None and parent(n, there[0], there[1]) == there[2]:
            found.append(edge)
    return found


def choose(index, low, branches):
    if len(branches) == 1:
        branches[0]()
        return
    half = len(branches) // 2
    pl.when(index < low + half)(lambda: choose(index, low, branches[:half]))
    pl.when(index >= low + half)(lambda: choose(index, low + half, branches[half:]))


def pick(index, values):
    result = values[0]
    for i, value in enumerate(values[1:], 1):
        result = jnp.where(index == i, value, result)
    return result


def split(order):
    before, steps, current = [], [], []
    for op in order:
        if op[0] == COMPUTE:
            before.append(current)
            steps.append(op[1:4])
            current = []
        else:
            current.append(op)
    return before, steps, current


def kernel(
    n, tok_hbm, gain_hbm, ids_hbm, weight_hbm, gate_hbm, up_hbm, down_hbm, out_ref,
    tok, gain, ids, weight, both, down, buf, own_shares, shares, part, srecv, rrecv,
    load_sem, w_s, w_r, ag_s, ag_r, ags_s, ags_r, rss_s, rss_r, rs_s, rs_r,
):
    ep = lax.axis_index("ep")
    z = lax.axis_index("tp")
    y, c = ep // 2, ep % 2
    rows, width = tok.shape
    inner = down.shape[0]
    experts = shares.shape[0]
    per = PIECES // UNITS
    tall = rows // UNITS
    short = rows // PIECES
    high = z // (n // 2)
    turn = 1 - 2 * high
    place = z + high * (n - 1 - 2 * z)
    sib = {"ep": 2 * y + 1 - c}
    toward = {ACROSS: {"ep": 2 * (1 - y) + c}, INWARD: {"tp": z + turn}, OUTWARD: {"tp": z - turn}}
    side = {ACROSS: 0, INWARD: 1 + high, OUTWARD: 2 - high}
    far_side = {ACROSS: 0, INWARD: 2 - high, OUTWARD: 1 + high}

    def block(row, at):
        return row + (1 - 2 * row) * y, at + high * (n - 1 - 2 * at)

    def remote(src, dst, send, recv, to):
        return pltpu.make_async_remote_copy(
            src_ref=src, dst_ref=dst, send_sem=send, recv_sem=recv, device_id=to, device_id_type=MESH
        )

    loads = [
        pltpu.make_async_copy(src, dst, load_sem.at[i])
        for i, (src, dst) in enumerate(
            (
                (tok_hbm, tok),
                (gain_hbm, gain),
                (ids_hbm, ids),
                (weight_hbm, weight),
                (gate_hbm.at[0], both.at[:, pl.ds(0, inner)]),
                (up_hbm.at[0], both.at[:, pl.ds(inner, inner)]),
                (down_hbm.at[0], down),
            )
        )
    ]
    for load in loads:
        load.start()

    barrier = pltpu.get_barrier_semaphore()
    for k in range(1, 4):
        pl.semaphore_signal(barrier, inc=1, device_id={"ep": (ep + k) % 4}, device_id_type=MESH)
    pl.semaphore_signal(barrier, inc=1, device_id=toward[INWARD], device_id_type=MESH)

    @pl.when(place > 0)
    def _():
        pl.semaphore_signal(barrier, inc=1, device_id=toward[OUTWARD], device_id_type=MESH)

    loads[0].wait()
    loads[1].wait()
    normed = norm_rows(tok[...], gain[...]).reshape(UNITS, per, short, width)
    for unit in range(UNITS):
        buf[y, z, unit, c] = normed[unit]
    loads[2].wait()
    loads[3].wait()
    for e in range(experts):
        named = jnp.where(ids[...] == e, weight[...], 0.0)
        total = named[0:1] + named[1:2]
        for k in range(n):
            own_shares[e, k : k + 1, :] = total[:, k * rows : (k + 1) * rows]

    pl.semaphore_wait(barrier, 4 + jnp.where(place > 0, 1, 0))

    def share(k):
        to = (ep + k) % 4
        return remote(own_shares.at[to], shares.at[ep], w_s.at[k], w_r.at[4 - k], {"ep": to})

    def copy_of(op):
        what, row, at, number, edge = op
        yb, zb = block(row, at)
        unit, piece = number // per, number % per
        if what == SEND:
            here = buf.at[yb, zb, unit, c, piece]
            return remote(here, here, ag_s.at[edge, yb, zb, number], ag_r.at[yb, zb, number], toward[edge])
        if what == RELAY:
            here = buf.at[yb, zb, unit, c, piece]
            return remote(here, here, ags_s.at[yb, zb, number], ags_r.at[yb, zb, number], sib)
        here = part.at[yb, zb, unit, c, piece]
        there = rrecv.at[far_side[edge], yb, zb, number]
        return remote(here, there, rs_s.at[yb, zb, number], rs_r.at[far_side[edge], yb, zb, number], toward[edge])

    def sum_copy(yb, zb, unit):
        return remote(part.at[yb, zb, unit, 1 - c], srecv.at[yb, zb, unit], rss_s.at[yb, zb, unit], rss_r.at[yb, zb, unit], sib)

    def run(here, ops, seen):
        for op in ops:
            what, row, at, number, edge = op
            yb, zb = block(row, at)
            unit, piece = number // per, number % per
            own = row == 0 and at == here
            if what == RELAY:
                if not own:
                    landed = buf.at[yb, zb, unit, c, piece]
                    remote(landed, landed, ags_s.at[yb, zb, number], ag_r.at[yb, zb, number], sib).wait_recv()
                copy_of(op).start()
            elif what == SEND:
                copy_of(op).start()
            else:
                if (row, at, unit) not in seen:
                    seen.add((row, at, unit))
                    sum_copy(yb, zb, unit).wait_recv()
                total = part[yb, zb, unit, c, piece].astype(jnp.float32)
                total = total + srecv[yb, zb, unit, piece].astype(jnp.float32)
                for child in children(n, here, (row, at, number)):
                    landed = rrecv.at[side[child], yb, zb, number]
                    remote(landed, landed, rs_s.at[yb, zb, number], rs_r.at[side[child], yb, zb, number], sib).wait_recv()
                    total = total + rrecv[side[child], yb, zb, number].astype(jnp.float32)
                if own:
                    out_ref[number * short : (number + 1) * short, :] = total.astype(out_ref.dtype)
                else:
                    part[yb, zb, unit, c, piece] = total.astype(jnp.bfloat16)
                    copy_of(op).start()

    plans = [split(order) for order in ORDER]
    steps = len(plans[0][1])
    branches, seen = [], [set() for _ in plans]
    for here, (before, _, _) in enumerate(plans):
        for ops in before:
            first = set()
            for op in ops:
                unit = (op[1], op[2], op[3] // per)
                if op[0] == REDUCE and unit not in seen[here]:
                    seen[here].add(unit)
                    first.add(unit)
            waited = {(r, a, u) for r in range(2) for a in range(n) for u in range(UNITS)} - first
            branches.append(functools.partial(run, here, ops, waited))

    def column(row):
        return jnp.transpose(jnp.broadcast_to(row, (rows, rows)))[:, :1]

    lane = lax.broadcasted_iota(jnp.int32, (8, rows), 1)

    def one(step, carry):
        choose(place * steps + step, 0, branches)

        @pl.when(step == 0)
        def _():
            for k in range(1, 4):
                share(k).start()
            shares[ep] = own_shares[ep]
            for k in range(1, 4):
                remote(own_shares.at[0], shares.at[(ep + k) % 4], w_s.at[k], w_r.at[k], sib).wait_recv()
            for load in loads[4:]:
                load.wait()

        row, at, unit = (
            pick(place, [pick(step, [s[i] for s in plan[1]]) for plan in plans]) for i in range(3)
        )
        yb, zb = block(row, at)
        for piece in range(per):
            landed = buf.at[yb, zb, unit, 1 - c, piece]
            number = unit * per + piece
            remote(landed, landed, ags_s.at[yb, zb, number], ags_r.at[yb, zb, number], sib).wait_recv()
        x = buf[yb, zb, unit].reshape(2 * tall, width)
        mixed = jnp.dot(x, both[...], preferred_element_type=jnp.float32)
        hidden = (jax.nn.silu(mixed[:, :inner]) * mixed[:, inner:]).astype(jnp.bfloat16)
        product = jnp.dot(hidden, down[...], preferred_element_type=jnp.float32)
        ours = [jnp.broadcast_to(shares[2 * yb + half, pl.ds(zb, 1), :], (8, rows)) for half in range(2)]
        turned = [pltpu.roll(values, tall, 1) for values in ours]
        first = jnp.where(lane < tall, ours[0], turned[1])
        second = jnp.where(lane < tall, turned[0], ours[1])
        w = column(jnp.where(unit == 0, first, second)[0:1])
        part[yb, zb, unit] = (product * w).astype(jnp.bfloat16).reshape(2, per, short, width)
        sum_copy(yb, zb, unit).start()
        return carry

    lax.fori_loop(0, steps, one, 0)

    def finish(here):
        after = plans[here][2]
        run(here, after, seen[here])
        for op in ORDER[here]:
            if op[0] in (RELAY, SEND) or (op[0] == REDUCE and parent(n, here, op[1:4]) is not None):
                copy_of(op).wait_send()

    choose(place, 0, [functools.partial(finish, here) for here in range(len(plans))])
    for k in range(1, 4):
        share(k).wait_send()
    for yb in range(2):
        for zb in range(n):
            for unit in range(UNITS):
                sum_copy(yb, zb, unit).wait_send()


def kernel_bytes(n, rows, width, inner):
    blocks = n * 4 + 2 * n * 2 + 2 * n + 6 * n + 4
    return 2 * width * (3 * inner + blocks * rows) + 16 * rows * (width + 2 * inner)


def fused_body(tokens, norm_gain, gate_weight, up_weight, down_weight, expert_ids, route_weight):
    rows, width = tokens.shape
    inner = gate_weight.shape[2]
    n = lax.axis_size("tp")
    experts = lax.axis_size("ep")
    vmem = pl.BlockSpec(memory_space=pltpu.VMEM)
    anywhere = pl.BlockSpec(memory_space=pl.ANY)
    dma = pltpu.SemaphoreType.DMA
    bf16 = jnp.bfloat16
    per, short = PIECES // UNITS, rows // PIECES
    return pl.pallas_call(
        functools.partial(kernel, n),
        out_shape=jax.ShapeDtypeStruct((rows, width), bf16),
        in_specs=[anywhere] * 7,
        out_specs=vmem,
        scratch_shapes=[
            pltpu.VMEM((rows, width), bf16),
            pltpu.VMEM((1, width), jnp.float32),
            pltpu.VMEM((TOP_K, n * rows), jnp.int32),
            pltpu.VMEM((TOP_K, n * rows), jnp.float32),
            pltpu.VMEM((width, 2 * inner), bf16),
            pltpu.VMEM((inner, width), bf16),
            pltpu.VMEM((2, n, UNITS, 2, per, short, width), bf16),
            pltpu.VMEM((experts, n, rows), jnp.float32),
            pltpu.VMEM((experts, n, rows), jnp.float32),
            pltpu.VMEM((2, n, UNITS, 2, per, short, width), bf16),
            pltpu.VMEM((2, n, UNITS, per, short, width), bf16),
            pltpu.VMEM((3, 2, n, PIECES, short, width), bf16),
            dma((7,)),
            dma((4,)),
            dma((4,)),
            dma((3, 2, n, PIECES)),
            dma((2, n, PIECES)),
            dma((2, n, PIECES)),
            dma((2, n, PIECES)),
            dma((2, n, UNITS)),
            dma((2, n, UNITS)),
            dma((2, n, PIECES)),
            dma((3, 2, n, PIECES)),
        ],
        compiler_params=pltpu.CompilerParams(
            collective_id=0, has_side_effects=True, vmem_limit_bytes=VMEM_ROOM
        ),
    )(tokens, norm_gain.reshape(1, width), expert_ids.T, route_weight.T, gate_weight, up_weight, down_weight)


def body(tokens, norm_gain, gate_weight, up_weight, down_weight, expert_ids, route_weight):
    rows, width = tokens.shape
    inner = gate_weight.shape[2]
    n = lax.axis_size("tp")
    fits = kernel_bytes(n, rows, width, inner) <= VMEM_ROOM and rows % 128 == 0
    chosen = plain_body
    if lax.axis_size("ep") == 4 and gate_weight.shape[0] == 1 and n == LINE and fits:
        chosen = fused_body
    return chosen(tokens, norm_gain, gate_weight, up_weight, down_weight, expert_ids, route_weight)


def solution(mesh):
    placed = (
        P(("grp", "ep", "tp"), None),
        P(),
        P("ep", None, "tp"),
        P("ep", None, "tp"),
        P("ep", "tp", None),
        P(("grp", "ep"), None),
        P(("grp", "ep"), None),
    )
    return jax.shard_map(
        body, mesh=mesh, in_specs=placed, out_specs=P(("grp", "ep", "tp"), None), check_vma=False
    )
```

```python
import functools

import jax
import jax.numpy as jnp
from jax import lax
from jax.experimental import pallas as pl
from jax.experimental.pallas import tpu as pltpu
from jax.sharding import PartitionSpec as P

TOP_K = 2
MESH = pl.DeviceIdType.MESH
VMEM_ROOM = 60 << 20

ACROSS, UP, DOWN = range(3)
RELAY, SEND, REDUCE, COMPUTE = range(4)
UNITS = 2
PIECES = 4
LINE = 4
SPREAD = ((11, 5, 14, 7), (11, 1, 7, 13), (15, 3, 8, 14), (11, 8, 13, 11))
GATHER = ((8, 11, 15, 1), (12, 14, 12, 11), (15, 12, 3, 3), (12, 5, 7, 1))
ORDER = (
    (
        (0, 0, 0, 0, 0), (0, 0, 0, 1, 0), (0, 0, 0, 2, 0), (0, 0, 0, 3, 0), (1, 0, 0, 0, 1), (1, 0, 0, 3, 0),
        (1, 0, 0, 1, 1), (1, 0, 0, 0, 0), (3, 0, 0, 0, 0), (1, 0, 0, 3, 1), (1, 0, 0, 1, 0), (3, 0, 0, 1, 0),
        (1, 0, 0, 2, 1), (0, 1, 0, 3, 0), (0, 0, 1, 3, 0), (1, 0, 1, 3, 0), (0, 1, 0, 0, 0), (0, 0, 1, 2, 0),
        (1, 0, 1, 2, 0), (0, 1, 0, 1, 0), (1, 1, 0, 1, 1), (3, 0, 1, 1, 0), (0, 0, 1, 1, 0), (0, 1, 1, 3, 0),
        (1, 0, 1, 1, 0), (1, 1, 1, 3, 1), (3, 1, 0, 0, 0), (2, 0, 1, 2, 1), (0, 0, 2, 2, 0), (0, 1, 1, 2, 0),
        (0, 0, 1, 0, 0), (1, 0, 1, 0, 0), (2, 1, 0, 0, 1), (2, 1, 0, 1, 0), (3, 1, 1, 1, 0), (0, 1, 1, 1, 0),
        (0, 0, 2, 0, 0), (1, 1, 1, 1, 1), (1, 0, 2, 0, 0), (3, 0, 1, 0, 0), (2, 1, 1, 2, 1), (2, 1, 1, 3, 0),
        (0, 0, 2, 1, 0), (0, 1, 1, 0, 0), (2, 0, 1, 1, 1), (0, 0, 3, 0, 0), (3, 0, 2, 0, 0), (2, 0, 1, 0, 1),
        (1, 0, 3, 0, 0), (3, 1, 1, 0, 0), (0, 0, 3, 2, 0), (0, 1, 2, 0, 0), (2, 0, 2, 1, 1), (1, 0, 2, 1, 0),
        (0, 0, 3, 3, 0), (1, 0, 3, 3, 0), (2, 1, 1, 1, 1), (3, 0, 3, 1, 0), (0, 1, 0, 2, 0), (0, 1, 3, 0, 0),
        (1, 0, 3, 2, 0), (2, 0, 1, 3, 1), (0, 1, 3, 1, 0), (0, 1, 2, 1, 0), (3, 1, 0, 1, 0), (0, 0, 3, 1, 0),
        (2, 1, 1, 0, 1), (3, 1, 3, 0, 0), (2, 1, 0, 2, 0), (0, 0, 2, 3, 0), (0, 1, 3, 3, 0), (3, 1, 2, 0, 0),
        (2, 1, 3, 0, 1), (2, 1, 3, 1, 0), (0, 1, 2, 2, 0), (0, 1, 3, 2, 0), (3, 0, 3, 0, 0), (2, 1, 2, 0, 0),
        (2, 1, 2, 1, 1), (0, 1, 2, 3, 0), (3, 1, 3, 1, 0), (2, 0, 3, 0, 1), (3, 0, 2, 1, 0), (2, 0, 3, 1, 1),
        (2, 1, 3, 2, 0), (3, 1, 2, 1, 0), (2, 0, 2, 0, 1), (2, 1, 3, 3, 0), (2, 1, 2, 3, 0), (2, 1, 2, 2, 0),
        (2, 0, 3, 2, 1), (2, 0, 3, 3, 1), (2, 0, 2, 3, 1), (2, 1, 0, 3, 0), (2, 0, 2, 2, 1), (2, 0, 0, 1, 0),
        (2, 0, 0, 3, 0), (2, 0, 0, 2, 0), (2, 0, 0, 0, 0),
    ),
    (
        (0, 0, 1, 1, 0), (0, 0, 1, 0, 0), (0, 0, 1, 2, 0), (0, 0, 1, 3, 0), (1, 0, 1, 3, 1), (1, 0, 1, 3, 2),
        (1, 0, 1, 0, 0), (1, 0, 1, 2, 1), (1, 0, 1, 2, 2), (1, 0, 1, 2, 0), (3, 0, 1, 0, 0), (1, 0, 1, 1, 2),
        (1, 0, 1, 0, 1), (3, 0, 1, 1, 0), (0, 0, 0, 0, 0), (0, 0, 2, 2, 0), (1, 0, 0, 0, 0), (0, 1, 1, 0, 0),
        (1, 0, 2, 2, 2), (1, 0, 0, 0, 1), (0, 0, 0, 1, 0), (1, 0, 0, 1, 1), (1, 0, 1, 0, 2), (0, 0, 2, 0, 0),
        (1, 0, 2, 0, 0), (0, 1, 1, 2, 0), (3, 0, 0, 0, 0), (0, 0, 0, 3, 0), (1, 0, 0, 3, 0), (1, 0, 0, 3, 1),
        (1, 0, 2, 0, 2), (0, 0, 2, 1, 0), (1, 0, 2, 1, 0), (0, 0, 0, 2, 0), (0, 1, 0, 0, 0), (1, 0, 0, 2, 1),
        (1, 0, 2, 1, 2), (3, 0, 2, 0, 0), (0, 0, 3, 0, 0), (0, 1, 2, 0, 0), (0, 1, 0, 1, 0), (1, 0, 0, 2, 0),
        (3, 0, 0, 1, 0), (0, 0, 2, 3, 0), (0, 1, 0, 3, 0), (1, 0, 3, 0, 2), (1, 0, 3, 0, 0), (1, 1, 0, 0, 1),
        (3, 1, 0, 0, 0), (0, 0, 3, 2, 0), (0, 1, 2, 1, 0), (0, 1, 1, 3, 0), (1, 0, 3, 2, 2), (1, 0, 2, 3, 0),
        (1, 1, 2, 1, 1), (3, 0, 2, 1, 0), (0, 0, 3, 3, 0), (0, 1, 0, 2, 0), (1, 0, 3, 3, 2), (3, 1, 2, 0, 0),
        (2, 1, 0, 0, 1), (0, 0, 3, 1, 0), (0, 1, 3, 0, 0), (1, 1, 0, 2, 2), (1, 0, 1, 1, 1), (3, 0, 3, 1, 0),
        (2, 1, 2, 0, 0), (0, 1, 1, 1, 0), (0, 1, 2, 3, 0), (0, 1, 3, 1, 0), (1, 1, 3, 1, 2), (1, 1, 1, 1, 1),
        (1, 0, 3, 3, 0), (3, 1, 0, 1, 0), (0, 1, 3, 2, 0), (1, 0, 3, 1, 2), (3, 1, 3, 0, 0), (1, 0, 2, 3, 2),
        (1, 1, 1, 0, 1), (2, 1, 0, 2, 0), (0, 1, 2, 2, 0), (3, 0, 3, 0, 0), (2, 1, 3, 1, 1), (1, 1, 2, 2, 2),
        (3, 1, 1, 0, 0), (0, 1, 3, 3, 0), (1, 1, 2, 3, 2), (3, 1, 1, 1, 0), (2, 0, 2, 1, 1), (3, 1, 3, 1, 0),
        (2, 1, 1, 1, 0), (2, 1, 1, 2, 1), (2, 1, 1, 3, 0), (3, 1, 2, 1, 0), (2, 1, 3, 2, 0), (2, 1, 3, 3, 2),
        (2, 1, 1, 0, 1), (2, 1, 0, 1, 0), (2, 1, 3, 0, 1), (2, 1, 2, 3, 0), (2, 1, 2, 1, 1), (2, 1, 2, 2, 0),
        (2, 0, 0, 3, 2), (2, 0, 3, 0, 1), (2, 1, 0, 3, 2), (2, 0, 3, 1, 1), (2, 0, 2, 0, 1), (2, 0, 0, 1, 2),
        (2, 0, 3, 2, 1), (2, 0, 0, 2, 2), (2, 0, 3, 3, 1), (2, 0, 0, 0, 2), (2, 0, 2, 3, 1), (2, 0, 1, 2, 0),
        (2, 0, 2, 2, 1), (2, 0, 1, 3, 0), (2, 0, 1, 1, 0), (2, 0, 1, 0, 0),
    ),
    (
        (1, 0, 2, 2, 2), (0, 0, 2, 2, 0), (0, 0, 2, 1, 0), (0, 0, 2, 0, 0), (0, 0, 2, 3, 0), (1, 0, 2, 2, 1),
        (1, 0, 2, 3, 0), (1, 0, 2, 0, 2), (1, 0, 2, 1, 1), (1, 0, 2, 0, 0), (3, 0, 2, 0, 0), (1, 0, 2, 0, 1),
        (1, 0, 2, 1, 2), (3, 0, 2, 1, 0), (0, 0, 3, 0, 0), (0, 0, 1, 3, 0), (0, 1, 2, 3, 0), (1, 0, 1, 3, 0),
        (1, 0, 3, 0, 2), (1, 0, 1, 3, 1), (1, 0, 2, 3, 2), (1, 0, 2, 3, 1), (0, 0, 1, 2, 0), (1, 0, 1, 2, 0),
        (0, 0, 3, 2, 0), (0, 1, 2, 0, 0), (1, 0, 3, 2, 0), (1, 0, 3, 2, 2), (3, 0, 1, 1, 0), (0, 0, 3, 3, 0),
        (0, 0, 1, 0, 0), (0, 1, 1, 3, 0), (1, 0, 1, 2, 1), (1, 0, 3, 3, 2), (1, 0, 1, 0, 1), (0, 0, 0, 0, 0),
        (0, 0, 3, 1, 0), (3, 0, 3, 1, 0), (0, 0, 0, 1, 0), (0, 1, 1, 2, 0), (0, 1, 3, 3, 0), (1, 0, 0, 0, 1),
        (1, 0, 0, 1, 0), (1, 0, 3, 1, 2), (3, 0, 3, 0, 0), (0, 0, 0, 3, 0), (0, 1, 3, 2, 0), (0, 1, 3, 1, 0),
        (1, 0, 0, 3, 0), (1, 1, 3, 1, 2), (1, 0, 0, 3, 1), (3, 0, 0, 0, 0), (0, 0, 0, 2, 0), (1, 0, 0, 2, 1),
        (1, 1, 3, 2, 2), (0, 1, 3, 0, 0), (1, 0, 0, 2, 0), (3, 1, 3, 1, 0), (0, 1, 0, 1, 0), (0, 1, 0, 0, 0),
        (1, 1, 0, 1, 1), (3, 0, 0, 1, 0), (0, 1, 2, 2, 0), (0, 1, 0, 3, 0), (1, 1, 2, 2, 2), (3, 1, 3, 0, 0),
        (0, 1, 2, 1, 0), (0, 1, 0, 2, 0), (1, 1, 0, 3, 1), (3, 1, 1, 1, 0), (2, 1, 3, 2, 0), (1, 0, 0, 1, 1),
        (3, 1, 0, 0, 0), (2, 1, 1, 3, 2), (1, 1, 1, 2, 1), (3, 1, 0, 1, 0), (2, 1, 0, 1, 2), (2, 1, 0, 0, 1),
        (0, 0, 1, 1, 0), (3, 1, 2, 1, 0), (2, 1, 0, 2, 0), (2, 1, 3, 3, 2), (0, 1, 1, 1, 0), (1, 1, 1, 1, 1),
        (3, 0, 1, 0, 0), (2, 1, 2, 3, 2), (0, 1, 1, 0, 0), (1, 0, 1, 1, 1), (3, 1, 2, 0, 0), (2, 1, 2, 2, 2),
        (2, 1, 3, 1, 0), (1, 1, 2, 1, 1), (3, 1, 1, 0, 0), (2, 1, 2, 0, 0), (2, 0, 0, 3, 2), (2, 1, 1, 2, 0),
        (2, 1, 1, 1, 0), (2, 1, 0, 3, 2), (2, 1, 1, 0, 0), (2, 0, 0, 1, 2), (2, 1, 3, 0, 0), (2, 0, 0, 2, 2),
        (2, 1, 2, 1, 0), (2, 0, 0, 0, 2), (2, 0, 1, 2, 2), (2, 0, 3, 0, 1), (2, 0, 3, 1, 1), (2, 0, 1, 3, 2),
        (2, 0, 1, 1, 2), (2, 0, 3, 2, 1), (2, 0, 1, 0, 2), (2, 0, 3, 3, 1), (2, 0, 2, 1, 0), (2, 0, 2, 3, 0),
        (2, 0, 2, 0, 0), (2, 0, 2, 2, 0),
    ),
    (
        (0, 0, 3, 0, 0), (0, 0, 3, 1, 0), (0, 0, 3, 2, 0), (0, 0, 3, 3, 0), (1, 0, 3, 0, 2), (1, 0, 3, 3, 0),
        (1, 0, 3, 2, 2), (1, 0, 3, 1, 0), (3, 0, 3, 0, 0), (1, 0, 3, 3, 2), (1, 0, 3, 0, 0), (3, 0, 3, 1, 0),
        (1, 0, 3, 1, 2), (1, 0, 3, 2, 0), (0, 0, 2, 2, 0), (0, 1, 3, 3, 0), (1, 1, 3, 3, 2), (1, 0, 2, 2, 0),
        (0, 1, 3, 1, 0), (0, 0, 2, 1, 0), (1, 1, 3, 1, 2), (0, 0, 2, 0, 0), (0, 1, 3, 0, 0), (1, 0, 2, 0, 0),
        (1, 1, 3, 0, 2), (3, 0, 2, 0, 0), (0, 0, 1, 3, 0), (0, 1, 3, 2, 0), (1, 0, 1, 3, 0), (3, 1, 3, 0, 0),
        (0, 1, 2, 2, 0), (0, 0, 2, 3, 0), (1, 0, 2, 3, 0), (1, 1, 2, 2, 2), (3, 1, 3, 1, 0), (2, 1, 3, 0, 0),
        (2, 1, 3, 1, 2), (0, 0, 1, 2, 0), (0, 1, 2, 0, 0), (3, 0, 2, 1, 0), (2, 1, 3, 2, 2), (0, 0, 1, 0, 0),
        (0, 1, 1, 3, 0), (1, 0, 1, 0, 0), (3, 0, 1, 1, 0), (2, 0, 2, 3, 2), (0, 0, 0, 0, 0), (0, 1, 2, 3, 0),
        (1, 0, 0, 0, 0), (2, 0, 2, 2, 2), (0, 0, 0, 3, 0), (3, 1, 2, 1, 0), (2, 1, 3, 3, 2), (0, 0, 0, 2, 0),
        (1, 0, 0, 2, 0), (0, 1, 1, 0, 0), (2, 1, 2, 3, 2), (3, 0, 0, 1, 0), (0, 1, 0, 0, 0), (0, 1, 0, 1, 0),
        (2, 1, 2, 2, 2), (0, 1, 0, 3, 0), (0, 1, 0, 2, 0), (3, 1, 0, 0, 0), (2, 0, 0, 3, 2), (0, 0, 0, 1, 0),
        (3, 1, 0, 1, 0), (2, 1, 0, 1, 0), (0, 1, 1, 2, 0), (3, 0, 0, 0, 0), (2, 1, 0, 2, 0), (2, 1, 0, 3, 2),
        (3, 1, 1, 1, 0), (2, 1, 0, 0, 0), (0, 1, 1, 1, 0), (2, 0, 0, 1, 2), (2, 1, 1, 2, 0), (3, 1, 1, 0, 0),
        (2, 1, 1, 3, 0), (2, 0, 0, 2, 2), (0, 0, 1, 1, 0), (0, 1, 2, 1, 0), (2, 1, 1, 1, 0), (2, 0, 0, 0, 2),
        (3, 0, 1, 0, 0), (2, 1, 1, 0, 0), (2, 0, 1, 2, 2), (3, 1, 2, 0, 0), (2, 0, 1, 3, 2), (2, 1, 2, 1, 0),
        (2, 1, 2, 0, 0), (2, 0, 1, 1, 2), (2, 0, 1, 0, 2), (2, 0, 2, 1, 2), (2, 0, 2, 0, 2), (2, 0, 3, 0, 0),
        (2, 0, 3, 1, 0), (2, 0, 3, 2, 0), (2, 0, 3, 3, 0),
    ),
)


def norm_rows(tokens, norm_gain):
    values = tokens.astype(jnp.float32)
    scaled = values * lax.rsqrt(jnp.mean(values * values, axis=-1, keepdims=True) + 1e-06)
    return (scaled * norm_gain).astype(jnp.bfloat16)


def expert_hidden(rows, gate_weight, up_weight):
    gate = jnp.einsum("e...d,edf->e...f", rows, gate_weight, preferred_element_type=jnp.float32)
    upper = jnp.einsum("e...d,edf->e...f", rows, up_weight, preferred_element_type=jnp.float32)
    return (jax.nn.silu(gate) * upper).astype(jnp.bfloat16)


def weigh_pieces(summed, weights):
    piece = lax.optimization_barrier(summed.astype(jnp.bfloat16)).astype(jnp.float32)
    total = piece[:, 0] * weights[:, 0:1]
    total = total + piece[:, 1] * weights[:, 1:2]
    return total.astype(jnp.bfloat16)


def plain_body(tokens, norm_gain, gate_weight, up_weight, down_weight, expert_ids, route_weight):
    tok_rows = tokens.shape[0]
    width = tokens.shape[1]
    local_experts = gate_weight.shape[0]
    inner = gate_weight.shape[2]
    n_tp = lax.axis_size("tp")
    n_ep = lax.axis_size("ep")
    experts = n_ep * local_experts
    most = max(2, tok_rows * TOP_K * 5 // (4 * experts))
    normed = norm_rows(tokens, norm_gain)
    flat_ids = expert_ids.reshape(n_tp, tok_rows * TOP_K)
    onehot = (flat_ids[:, :, None] == jnp.arange(experts, dtype=jnp.int32)[None, None, :]).astype(
        jnp.int32
    )
    before = jnp.cumsum(onehot, axis=1) - onehot
    slots = jnp.sum(before * onehot, axis=-1)
    owner = jnp.arange(n_tp, dtype=jnp.int32)[:, None]
    row_index = (flat_ids * (n_tp * most) + owner * most + slots).reshape(-1)
    mine = lax.axis_index("tp")
    own_ids = lax.dynamic_slice_in_dim(flat_ids, mine, 1, 0)[0]
    own_slots = lax.dynamic_slice_in_dim(slots, mine, 1, 0)[0]
    own_index = own_ids * most + own_slots
    whole = lax.all_gather(normed, "tp", axis=0, tiled=True)
    sending = (
        jnp.zeros((experts * n_tp * most, width), jnp.bfloat16)
        .at[row_index]
        .set(jnp.repeat(whole, TOP_K, axis=0))
    )
    arrived = lax.all_to_all(
        sending.reshape(experts, n_tp * most, width), "ep", split_axis=0, concat_axis=1, tiled=True
    )
    hidden = expert_hidden(arrived, gate_weight, up_weight)
    by_source = hidden.reshape(local_experts, n_ep, n_tp, most, inner).transpose(2, 0, 1, 3, 4)
    per_device = local_experts * n_ep * most
    product = jnp.einsum(
        "tlnmf,lfd->tlnmd", by_source, down_weight, preferred_element_type=jnp.float32
    )
    own_sums = lax.psum_scatter(
        product.astype(jnp.bfloat16)
        .astype(jnp.float32)
        .reshape(per_device * lax.axis_size("tp"), width)
        .astype(jnp.bfloat16),
        "tp",
        scatter_dimension=0,
        tiled=True,
    )
    own_pieces = own_sums.reshape(local_experts, n_ep, most, width)
    back = lax.all_to_all(own_pieces, "ep", split_axis=1, concat_axis=0, tiled=True)
    picked = back.reshape(experts * most, width)[own_index].reshape(tok_rows, TOP_K, width)
    own_weights = lax.dynamic_slice_in_dim(route_weight, mine * tok_rows, tok_rows, 0)
    return weigh_pieces(picked.astype(jnp.float32), own_weights)


def neighbour(n, place, edge, piece):
    row, at, number = piece
    if edge == ACROSS:
        return place, (1 - row, at, number), ACROSS
    there = place + (1 if edge == UP else -1)
    return (there, piece, DOWN if edge == UP else UP) if 0 <= there < n else None


def parent(n, crossings, place, piece):
    row, at, number = piece
    goal = at
    if row:
        bits = crossings[at][number]
        places = [k for k in range(n) if bits >> k & 1]
        goal = min(places, key=lambda k: (abs(k - place), abs(k - at)))
    if goal == place:
        return ACROSS if row else None
    return UP if goal > place else DOWN


def children(n, crossings, place, piece):
    found = []
    for edge in (ACROSS, UP, DOWN):
        there = neighbour(n, place, edge, piece)
        if there is not None and parent(n, crossings, there[0], there[1]) == there[2]:
            found.append(edge)
    return found


def choose(index, low, branches):
    if len(branches) == 1:
        branches[0]()
        return
    half = len(branches) // 2
    pl.when(index < low + half)(lambda: choose(index, low, branches[:half]))
    pl.when(index >= low + half)(lambda: choose(index, low + half, branches[half:]))


def pick(index, values):
    result = values[0]
    for i, value in enumerate(values[1:], 1):
        result = jnp.where(index == i, value, result)
    return result


def split(order):
    before, steps, current = [], [], []
    for op in order:
        if op[0] == COMPUTE:
            before.append(current)
            steps.append(op[1:4])
            current = []
        else:
            current.append(op)
    return before, steps, current


def kernel(
    n, tok_hbm, gain_hbm, ids_hbm, weight_hbm, gate_hbm, up_hbm, down_hbm, out_ref,
    tok, gain, ids, weight, both, down, buf, own_shares, shares, part, srecv, rrecv,
    load_sem, w_s, w_r, sib_s, ag_s, rs_s, ag_r, ags_r, rss_r, rs_r,
):
    ep = lax.axis_index("ep")
    z = lax.axis_index("tp")
    y, c = ep // 2, ep % 2
    rows, width = tok.shape
    inner = down.shape[0]
    experts = shares.shape[0]
    per = PIECES // UNITS
    tall = rows // UNITS
    short = rows // PIECES
    sib = {"ep": 2 * y + 1 - c}
    toward = {ACROSS: {"ep": 2 * (1 - y) + c}, UP: {"tp": z + 1}, DOWN: {"tp": z - 1}}

    def row_of(row):
        return row + (1 - 2 * row) * y

    def first(row, at, unit, lane):
        return (((row * n + at) * UNITS + unit) * 2 + lane) * per

    def remote(src, dst, send, recv, to):
        return pltpu.make_async_remote_copy(
            src_ref=src, dst_ref=dst, send_sem=send, recv_sem=recv, device_id=to, device_id_type=MESH
        )

    loads = [
        pltpu.make_async_copy(src, dst, load_sem.at[i])
        for i, (src, dst) in enumerate(
            (
                (tok_hbm, tok),
                (gain_hbm, gain),
                (ids_hbm, ids),
                (weight_hbm, weight),
                (gate_hbm.at[0], both.at[:, pl.ds(0, inner)]),
                (up_hbm.at[0], both.at[:, pl.ds(inner, inner)]),
                (down_hbm.at[0], down),
            )
        )
    ]
    for load in loads:
        load.start()

    barrier = pltpu.get_barrier_semaphore()
    for k in range(1, 4):
        pl.semaphore_signal(barrier, inc=1, device_id={"ep": (ep + k) % 4}, device_id_type=MESH)

    @pl.when(z < n - 1)
    def _():
        pl.semaphore_signal(barrier, inc=1, device_id=toward[UP], device_id_type=MESH)

    @pl.when(z > 0)
    def _():
        pl.semaphore_signal(barrier, inc=1, device_id=toward[DOWN], device_id_type=MESH)

    loads[0].wait()
    loads[1].wait()
    normed = norm_rows(tok[...], gain[...]).reshape(UNITS, per, short, width)
    for unit in range(UNITS):
        buf[pl.ds(first(y, z, unit, c), per)] = normed[unit]
    loads[2].wait()
    loads[3].wait()
    for e in range(experts):
        named = jnp.where(ids[...] == e, weight[...], 0.0)
        total = named[0:1] + named[1:2]
        for k in range(n):
            own_shares[e, k : k + 1, :] = total[:, k * rows : (k + 1) * rows]

    pl.semaphore_wait(barrier, 3 + jnp.where(z > 0, 1, 0) + jnp.where(z < n - 1, 1, 0))

    def share(k):
        to = (ep + k) % 4
        return remote(own_shares.at[to], shares.at[ep], w_s, w_r, {"ep": to})

    def held(yb, at, number, lane):
        return buf.at[first(yb, at, number // per, lane) + number % per]

    def sum_copy(yb, at, unit):
        return remote(part.at[yb, at, unit, 1 - c], srecv.at[yb, at, unit], sib_s, rss_r.at[yb, at, unit], sib)

    def run(here, ops, waited):
        waited = set(waited)
        for op in ops:
            what, row, at, number, edge = op
            yb = row_of(row)
            unit, piece = number // per, number % per
            mine = held(yb, at, number, c)
            own = row == 0 and at == here
            if what == RELAY:
                if not own:
                    remote(mine, mine, ag_s, ag_r.at[yb, at, number], sib).wait_recv()
                remote(mine, mine, sib_s, ags_r.at[yb, at, unit], sib).start()
            elif what == SEND:
                remote(mine, mine, ag_s, ag_r.at[yb, at, number], toward[edge]).start()
            else:
                if (row, at, unit) not in waited:
                    waited.add((row, at, unit))
                    sum_copy(yb, at, unit).wait_recv()
                total = part[yb, at, unit, c, piece].astype(jnp.float32)
                total = total + srecv[yb, at, unit, piece].astype(jnp.float32)
                count = len(children(n, GATHER, here, (row, at, number)))
                if count:
                    landed = rrecv.at[yb, at, number, pl.ds(0, count)]
                    remote(landed, landed, rs_s, rs_r.at[yb, at, number], sib).wait_recv()
                for slot in range(count):
                    total = total + rrecv[yb, at, number, slot].astype(jnp.float32)
                if own:
                    out_ref[number * short : (number + 1) * short, :] = total.astype(out_ref.dtype)
                else:
                    part[yb, at, unit, c, piece] = total.astype(jnp.bfloat16)
                    there, seen_as, back = neighbour(n, here, edge, (row, at, number))
                    slot = children(n, GATHER, there, seen_as).index(back)
                    remote(
                        part.at[yb, at, unit, c, piece], rrecv.at[yb, at, number, slot],
                        rs_s, rs_r.at[yb, at, number], toward[edge],
                    ).start()

    plans = [split(order) for order in ORDER]
    steps = len(plans[0][1])
    branches, waited = [], [set() for _ in plans]
    for here, (before, _, _) in enumerate(plans):
        for ops in before:
            branches.append(functools.partial(run, here, ops, waited[here]))
            waited[here] = waited[here] | {(op[1], op[2], op[3] // per) for op in ops if op[0] == REDUCE}

    def column(row):
        return jnp.transpose(jnp.broadcast_to(row, (rows, rows)))[:, :1]

    lane = lax.broadcasted_iota(jnp.int32, (8, rows), 1)

    def one(step, carry):
        choose(z * steps + step, 0, branches)

        @pl.when(step == 0)
        def _():
            for k in range(1, 4):
                share(k).start()
            shares[ep] = own_shares[ep]
            remote(own_shares.at[pl.ds(0, 3)], shares.at[pl.ds(0, 3)], w_s, w_r, sib).wait_recv()
            for load in loads[4:]:
                load.wait()

        row, at, unit = (
            pick(z, [pick(step, [s[i] for s in plan[1]]) for plan in plans]) for i in range(3)
        )
        yb = row_of(row)
        theirs = buf.at[pl.ds(first(yb, at, unit, 1 - c), per)]
        remote(theirs, theirs, sib_s, ags_r.at[yb, at, unit], sib).wait_recv()
        x = buf[pl.ds(first(yb, at, unit, 0), 2 * per)].reshape(2 * tall, width)
        mixed = jnp.dot(x, both[...], preferred_element_type=jnp.float32)
        hidden = (jax.nn.silu(mixed[:, :inner]) * mixed[:, inner:]).astype(jnp.bfloat16)
        product = jnp.dot(hidden, down[...], preferred_element_type=jnp.float32)
        ours = [jnp.broadcast_to(shares[2 * yb + half, pl.ds(at, 1), :], (8, rows)) for half in range(2)]
        turned = [pltpu.roll(values, tall, 1) for values in ours]
        early = jnp.where(lane < tall, ours[0], turned[1])
        late = jnp.where(lane < tall, turned[0], ours[1])
        w = column(jnp.where(unit == 0, early, late)[0:1])
        part[yb, at, unit] = (product * w).astype(jnp.bfloat16).reshape(2, per, short, width)
        sum_copy(yb, at, unit).start()
        return carry

    lax.fori_loop(0, steps, one, 0)

    def finish(here):
        run(here, plans[here][2], waited[here])
        for what, sem in ((SEND, ag_s), (REDUCE, rs_s)):
            count = sum(op[0] == what and (what == SEND or op[1] > 0 or op[2] != here) for op in ORDER[here])
            sent = buf.at[pl.ds(0, count)]
            remote(sent, sent, sem, sem, sib).wait_send()

    choose(z, 0, [functools.partial(finish, here) for here in range(len(plans))])
    remote(buf, buf, sib_s, sib_s, sib).wait_send()
    remote(own_shares.at[pl.ds(0, 3)], shares.at[pl.ds(0, 3)], w_s, w_r, sib).wait_send()


def kernel_bytes(n, rows, width, inner):
    blocks = n * 4 + 2 * n * 2 + 2 * n + 6 * n + 4
    return 2 * width * (3 * inner + blocks * rows) + 16 * rows * (width + 2 * inner)


def fused_body(tokens, norm_gain, gate_weight, up_weight, down_weight, expert_ids, route_weight):
    rows, width = tokens.shape
    inner = gate_weight.shape[2]
    n = lax.axis_size("tp")
    experts = lax.axis_size("ep")
    vmem = pl.BlockSpec(memory_space=pltpu.VMEM)
    anywhere = pl.BlockSpec(memory_space=pl.ANY)
    dma = pltpu.SemaphoreType.DMA
    bf16 = jnp.bfloat16
    per, short = PIECES // UNITS, rows // PIECES
    return pl.pallas_call(
        functools.partial(kernel, n),
        out_shape=jax.ShapeDtypeStruct((rows, width), bf16),
        in_specs=[anywhere] * 7,
        out_specs=vmem,
        scratch_shapes=[
            pltpu.VMEM((rows, width), bf16),
            pltpu.VMEM((1, width), jnp.float32),
            pltpu.VMEM((TOP_K, n * rows), jnp.int32),
            pltpu.VMEM((TOP_K, n * rows), jnp.float32),
            pltpu.VMEM((width, 2 * inner), bf16),
            pltpu.VMEM((inner, width), bf16),
            pltpu.VMEM((2 * n * UNITS * 2 * per, short, width), bf16),
            pltpu.VMEM((experts, n, rows), jnp.float32),
            pltpu.VMEM((experts, n, rows), jnp.float32),
            pltpu.VMEM((2, n, UNITS, 2, per, short, width), bf16),
            pltpu.VMEM((2, n, UNITS, per, short, width), bf16),
            pltpu.VMEM((2, n, PIECES, 3, short, width), bf16),
            dma((7,)),
            dma,
            dma,
            dma,
            dma,
            dma,
            dma((2, n, PIECES)),
            dma((2, n, UNITS)),
            dma((2, n, UNITS)),
            dma((2, n, PIECES)),
        ],
        compiler_params=pltpu.CompilerParams(
            collective_id=0, has_side_effects=True, vmem_limit_bytes=VMEM_ROOM
        ),
    )(tokens, norm_gain.reshape(1, width), expert_ids.T, route_weight.T, gate_weight, up_weight, down_weight)


def body(tokens, norm_gain, gate_weight, up_weight, down_weight, expert_ids, route_weight):
    rows, width = tokens.shape
    inner = gate_weight.shape[2]
    n = lax.axis_size("tp")
    fits = kernel_bytes(n, rows, width, inner) <= VMEM_ROOM and rows % 128 == 0
    chosen = plain_body
    if lax.axis_size("ep") == 4 and gate_weight.shape[0] == 1 and n == LINE and fits:
        chosen = fused_body
    return chosen(tokens, norm_gain, gate_weight, up_weight, down_weight, expert_ids, route_weight)


def solution(mesh):
    placed = (
        P(("grp", "ep", "tp"), None),
        P(),
        P("ep", None, "tp"),
        P("ep", None, "tp"),
        P("ep", "tp", None),
        P(("grp", "ep"), None),
        P(("grp", "ep"), None),
    )
    return jax.shard_map(
        body, mesh=mesh, in_specs=placed, out_specs=P(("grp", "ep", "tp"), None), check_vma=False
    )
```

```python
import functools

import jax
import jax.numpy as jnp
from jax import lax
from jax.experimental import pallas as pl
from jax.experimental.pallas import tpu as pltpu
from jax.sharding import PartitionSpec as P

TOP_K = 2
MESH = pl.DeviceIdType.MESH
VMEM_ROOM = 60 << 20

ACROSS, UP, DOWN = range(3)
RELAY, SEND, REDUCE, COMPUTE = range(4)
UNITS = 2
PIECES = 4
PHASES = 1
LINE = 4
SPREAD = ((11, 5, 14, 7), (11, 1, 7, 13), (15, 3, 8, 14), (11, 8, 13, 11))
GATHER = ((8, 11, 15, 1), (12, 14, 12, 11), (15, 12, 3, 3), (12, 5, 7, 1))
ORDER = (
    (
        (0, 0, 0, 0, 0), (0, 0, 0, 1, 0), (0, 0, 0, 2, 0), (0, 0, 0, 3, 0), (1, 0, 0, 0, 1), (1, 0, 0, 3, 0),
        (1, 0, 0, 1, 1), (1, 0, 0, 0, 0), (3, 0, 0, 0, 0), (1, 0, 0, 3, 1), (1, 0, 0, 1, 0), (3, 0, 0, 1, 0),
        (1, 0, 0, 2, 1), (0, 1, 0, 3, 0), (0, 0, 1, 3, 0), (1, 0, 1, 3, 0), (0, 1, 0, 0, 0), (0, 0, 1, 2, 0),
        (1, 0, 1, 2, 0), (0, 1, 0, 1, 0), (1, 1, 0, 1, 1), (3, 0, 1, 1, 0), (0, 0, 1, 1, 0), (0, 1, 1, 3, 0),
        (1, 0, 1, 1, 0), (1, 1, 1, 3, 1), (3, 1, 0, 0, 0), (2, 0, 1, 2, 1), (0, 0, 2, 2, 0), (0, 1, 1, 2, 0),
        (0, 0, 1, 0, 0), (1, 0, 1, 0, 0), (2, 1, 0, 0, 1), (2, 1, 0, 1, 0), (3, 1, 1, 1, 0), (0, 1, 1, 1, 0),
        (0, 0, 2, 0, 0), (1, 1, 1, 1, 1), (1, 0, 2, 0, 0), (3, 0, 1, 0, 0), (2, 1, 1, 2, 1), (2, 1, 1, 3, 0),
        (0, 0, 2, 1, 0), (0, 1, 1, 0, 0), (2, 0, 1, 1, 1), (0, 0, 3, 0, 0), (3, 0, 2, 0, 0), (2, 0, 1, 0, 1),
        (1, 0, 3, 0, 0), (3, 1, 1, 0, 0), (0, 0, 3, 2, 0), (0, 1, 2, 0, 0), (2, 0, 2, 1, 1), (1, 0, 2, 1, 0),
        (0, 0, 3, 3, 0), (1, 0, 3, 3, 0), (2, 1, 1, 1, 1), (3, 0, 3, 1, 0), (0, 1, 0, 2, 0), (0, 1, 3, 0, 0),
        (1, 0, 3, 2, 0), (2, 0, 1, 3, 1), (0, 1, 3, 1, 0), (0, 1, 2, 1, 0), (3, 1, 0, 1, 0), (0, 0, 3, 1, 0),
        (2, 1, 1, 0, 1), (3, 1, 3, 0, 0), (2, 1, 0, 2, 0), (0, 0, 2, 3, 0), (0, 1, 3, 3, 0), (3, 1, 2, 0, 0),
        (2, 1, 3, 0, 1), (2, 1, 3, 1, 0), (0, 1, 2, 2, 0), (0, 1, 3, 2, 0), (3, 0, 3, 0, 0), (2, 1, 2, 0, 0),
        (2, 1, 2, 1, 1), (0, 1, 2, 3, 0), (3, 1, 3, 1, 0), (2, 0, 3, 0, 1), (3, 0, 2, 1, 0), (2, 0, 3, 1, 1),
        (2, 1, 3, 2, 0), (3, 1, 2, 1, 0), (2, 0, 2, 0, 1), (2, 1, 3, 3, 0), (2, 1, 2, 3, 0), (2, 1, 2, 2, 0),
        (2, 0, 3, 2, 1), (2, 0, 3, 3, 1), (2, 0, 2, 3, 1), (2, 1, 0, 3, 0), (2, 0, 2, 2, 1), (2, 0, 0, 1, 0),
        (2, 0, 0, 3, 0), (2, 0, 0, 2, 0), (2, 0, 0, 0, 0),
    ),
    (
        (0, 0, 1, 1, 0), (0, 0, 1, 0, 0), (0, 0, 1, 2, 0), (0, 0, 1, 3, 0), (1, 0, 1, 3, 1), (1, 0, 1, 3, 2),
        (1, 0, 1, 0, 0), (1, 0, 1, 2, 1), (1, 0, 1, 2, 2), (1, 0, 1, 2, 0), (3, 0, 1, 0, 0), (1, 0, 1, 1, 2),
        (1, 0, 1, 0, 1), (3, 0, 1, 1, 0), (0, 0, 0, 0, 0), (0, 0, 2, 2, 0), (1, 0, 0, 0, 0), (0, 1, 1, 0, 0),
        (1, 0, 2, 2, 2), (1, 0, 0, 0, 1), (0, 0, 0, 1, 0), (1, 0, 0, 1, 1), (1, 0, 1, 0, 2), (0, 0, 2, 0, 0),
        (1, 0, 2, 0, 0), (0, 1, 1, 2, 0), (3, 0, 0, 0, 0), (0, 0, 0, 3, 0), (1, 0, 0, 3, 0), (1, 0, 0, 3, 1),
        (1, 0, 2, 0, 2), (0, 0, 2, 1, 0), (1, 0, 2, 1, 0), (0, 0, 0, 2, 0), (0, 1, 0, 0, 0), (1, 0, 0, 2, 1),
        (1, 0, 2, 1, 2), (3, 0, 2, 0, 0), (0, 0, 3, 0, 0), (0, 1, 2, 0, 0), (0, 1, 0, 1, 0), (1, 0, 0, 2, 0),
        (3, 0, 0, 1, 0), (0, 0, 2, 3, 0), (0, 1, 0, 3, 0), (1, 0, 3, 0, 2), (1, 0, 3, 0, 0), (1, 1, 0, 0, 1),
        (3, 1, 0, 0, 0), (0, 0, 3, 2, 0), (0, 1, 2, 1, 0), (0, 1, 1, 3, 0), (1, 0, 3, 2, 2), (1, 0, 2, 3, 0),
        (1, 1, 2, 1, 1), (3, 0, 2, 1, 0), (0, 0, 3, 3, 0), (0, 1, 0, 2, 0), (1, 0, 3, 3, 2), (3, 1, 2, 0, 0),
        (2, 1, 0, 0, 1), (0, 0, 3, 1, 0), (0, 1, 3, 0, 0), (1, 1, 0, 2, 2), (1, 0, 1, 1, 1), (3, 0, 3, 1, 0),
        (2, 1, 2, 0, 0), (0, 1, 1, 1, 0), (0, 1, 2, 3, 0), (0, 1, 3, 1, 0), (1, 1, 3, 1, 2), (1, 1, 1, 1, 1),
        (1, 0, 3, 3, 0), (3, 1, 0, 1, 0), (0, 1, 3, 2, 0), (1, 0, 3, 1, 2), (3, 1, 3, 0, 0), (1, 0, 2, 3, 2),
        (1, 1, 1, 0, 1), (2, 1, 0, 2, 0), (0, 1, 2, 2, 0), (3, 0, 3, 0, 0), (2, 1, 3, 1, 1), (1, 1, 2, 2, 2),
        (3, 1, 1, 0, 0), (0, 1, 3, 3, 0), (1, 1, 2, 3, 2), (3, 1, 1, 1, 0), (2, 0, 2, 1, 1), (3, 1, 3, 1, 0),
        (2, 1, 1, 1, 0), (2, 1, 1, 2, 1), (2, 1, 1, 3, 0), (3, 1, 2, 1, 0), (2, 1, 3, 2, 0), (2, 1, 3, 3, 2),
        (2, 1, 1, 0, 1), (2, 1, 0, 1, 0), (2, 1, 3, 0, 1), (2, 1, 2, 3, 0), (2, 1, 2, 1, 1), (2, 1, 2, 2, 0),
        (2, 0, 0, 3, 2), (2, 0, 3, 0, 1), (2, 1, 0, 3, 2), (2, 0, 3, 1, 1), (2, 0, 2, 0, 1), (2, 0, 0, 1, 2),
        (2, 0, 3, 2, 1), (2, 0, 0, 2, 2), (2, 0, 3, 3, 1), (2, 0, 0, 0, 2), (2, 0, 2, 3, 1), (2, 0, 1, 2, 0),
        (2, 0, 2, 2, 1), (2, 0, 1, 3, 0), (2, 0, 1, 1, 0), (2, 0, 1, 0, 0),
    ),
    (
        (1, 0, 2, 2, 2), (0, 0, 2, 2, 0), (0, 0, 2, 1, 0), (0, 0, 2, 0, 0), (0, 0, 2, 3, 0), (1, 0, 2, 2, 1),
        (1, 0, 2, 3, 0), (1, 0, 2, 0, 2), (1, 0, 2, 1, 1), (1, 0, 2, 0, 0), (3, 0, 2, 0, 0), (1, 0, 2, 0, 1),
        (1, 0, 2, 1, 2), (3, 0, 2, 1, 0), (0, 0, 3, 0, 0), (0, 0, 1, 3, 0), (0, 1, 2, 3, 0), (1, 0, 1, 3, 0),
        (1, 0, 3, 0, 2), (1, 0, 1, 3, 1), (1, 0, 2, 3, 2), (1, 0, 2, 3, 1), (0, 0, 1, 2, 0), (1, 0, 1, 2, 0),
        (0, 0, 3, 2, 0), (0, 1, 2, 0, 0), (1, 0, 3, 2, 0), (1, 0, 3, 2, 2), (3, 0, 1, 1, 0), (0, 0, 3, 3, 0),
        (0, 0, 1, 0, 0), (0, 1, 1, 3, 0), (1, 0, 1, 2, 1), (1, 0, 3, 3, 2), (1, 0, 1, 0, 1), (0, 0, 0, 0, 0),
        (0, 0, 3, 1, 0), (3, 0, 3, 1, 0), (0, 0, 0, 1, 0), (0, 1, 1, 2, 0), (0, 1, 3, 3, 0), (1, 0, 0, 0, 1),
        (1, 0, 0, 1, 0), (1, 0, 3, 1, 2), (3, 0, 3, 0, 0), (0, 0, 0, 3, 0), (0, 1, 3, 2, 0), (0, 1, 3, 1, 0),
        (1, 0, 0, 3, 0), (1, 1, 3, 1, 2), (1, 0, 0, 3, 1), (3, 0, 0, 0, 0), (0, 0, 0, 2, 0), (1, 0, 0, 2, 1),
        (1, 1, 3, 2, 2), (0, 1, 3, 0, 0), (1, 0, 0, 2, 0), (3, 1, 3, 1, 0), (0, 1, 0, 1, 0), (0, 1, 0, 0, 0),
        (1, 1, 0, 1, 1), (3, 0, 0, 1, 0), (0, 1, 2, 2, 0), (0, 1, 0, 3, 0), (1, 1, 2, 2, 2), (3, 1, 3, 0, 0),
        (0, 1, 2, 1, 0), (0, 1, 0, 2, 0), (1, 1, 0, 3, 1), (3, 1, 1, 1, 0), (2, 1, 3, 2, 0), (1, 0, 0, 1, 1),
        (3, 1, 0, 0, 0), (2, 1, 1, 3, 2), (1, 1, 1, 2, 1), (3, 1, 0, 1, 0), (2, 1, 0, 1, 2), (2, 1, 0, 0, 1),
        (0, 0, 1, 1, 0), (3, 1, 2, 1, 0), (2, 1, 0, 2, 0), (2, 1, 3, 3, 2), (0, 1, 1, 1, 0), (1, 1, 1, 1, 1),
        (3, 0, 1, 0, 0), (2, 1, 2, 3, 2), (0, 1, 1, 0, 0), (1, 0, 1, 1, 1), (3, 1, 2, 0, 0), (2, 1, 2, 2, 2),
        (2, 1, 3, 1, 0), (1, 1, 2, 1, 1), (3, 1, 1, 0, 0), (2, 1, 2, 0, 0), (2, 0, 0, 3, 2), (2, 1, 1, 2, 0),
        (2, 1, 1, 1, 0), (2, 1, 0, 3, 2), (2, 1, 1, 0, 0), (2, 0, 0, 1, 2), (2, 1, 3, 0, 0), (2, 0, 0, 2, 2),
        (2, 1, 2, 1, 0), (2, 0, 0, 0, 2), (2, 0, 1, 2, 2), (2, 0, 3, 0, 1), (2, 0, 3, 1, 1), (2, 0, 1, 3, 2),
        (2, 0, 1, 1, 2), (2, 0, 3, 2, 1), (2, 0, 1, 0, 2), (2, 0, 3, 3, 1), (2, 0, 2, 1, 0), (2, 0, 2, 3, 0),
        (2, 0, 2, 0, 0), (2, 0, 2, 2, 0),
    ),
    (
        (0, 0, 3, 0, 0), (0, 0, 3, 1, 0), (0, 0, 3, 2, 0), (0, 0, 3, 3, 0), (1, 0, 3, 0, 2), (1, 0, 3, 3, 0),
        (1, 0, 3, 2, 2), (1, 0, 3, 1, 0), (3, 0, 3, 0, 0), (1, 0, 3, 3, 2), (1, 0, 3, 0, 0), (3, 0, 3, 1, 0),
        (1, 0, 3, 1, 2), (1, 0, 3, 2, 0), (0, 0, 2, 2, 0), (0, 1, 3, 3, 0), (1, 1, 3, 3, 2), (1, 0, 2, 2, 0),
        (0, 1, 3, 1, 0), (0, 0, 2, 1, 0), (1, 1, 3, 1, 2), (0, 0, 2, 0, 0), (0, 1, 3, 0, 0), (1, 0, 2, 0, 0),
        (1, 1, 3, 0, 2), (3, 0, 2, 0, 0), (0, 0, 1, 3, 0), (0, 1, 3, 2, 0), (1, 0, 1, 3, 0), (3, 1, 3, 0, 0),
        (0, 1, 2, 2, 0), (0, 0, 2, 3, 0), (1, 0, 2, 3, 0), (1, 1, 2, 2, 2), (3, 1, 3, 1, 0), (2, 1, 3, 0, 0),
        (2, 1, 3, 1, 2), (0, 0, 1, 2, 0), (0, 1, 2, 0, 0), (3, 0, 2, 1, 0), (2, 1, 3, 2, 2), (0, 0, 1, 0, 0),
        (0, 1, 1, 3, 0), (1, 0, 1, 0, 0), (3, 0, 1, 1, 0), (2, 0, 2, 3, 2), (0, 0, 0, 0, 0), (0, 1, 2, 3, 0),
        (1, 0, 0, 0, 0), (2, 0, 2, 2, 2), (0, 0, 0, 3, 0), (3, 1, 2, 1, 0), (2, 1, 3, 3, 2), (0, 0, 0, 2, 0),
        (1, 0, 0, 2, 0), (0, 1, 1, 0, 0), (2, 1, 2, 3, 2), (3, 0, 0, 1, 0), (0, 1, 0, 0, 0), (0, 1, 0, 1, 0),
        (2, 1, 2, 2, 2), (0, 1, 0, 3, 0), (0, 1, 0, 2, 0), (3, 1, 0, 0, 0), (2, 0, 0, 3, 2), (0, 0, 0, 1, 0),
        (3, 1, 0, 1, 0), (2, 1, 0, 1, 0), (0, 1, 1, 2, 0), (3, 0, 0, 0, 0), (2, 1, 0, 2, 0), (2, 1, 0, 3, 2),
        (3, 1, 1, 1, 0), (2, 1, 0, 0, 0), (0, 1, 1, 1, 0), (2, 0, 0, 1, 2), (2, 1, 1, 2, 0), (3, 1, 1, 0, 0),
        (2, 1, 1, 3, 0), (2, 0, 0, 2, 2), (0, 0, 1, 1, 0), (0, 1, 2, 1, 0), (2, 1, 1, 1, 0), (2, 0, 0, 0, 2),
        (3, 0, 1, 0, 0), (2, 1, 1, 0, 0), (2, 0, 1, 2, 2), (3, 1, 2, 0, 0), (2, 0, 1, 3, 2), (2, 1, 2, 1, 0),
        (2, 1, 2, 0, 0), (2, 0, 1, 1, 2), (2, 0, 1, 0, 2), (2, 0, 2, 1, 2), (2, 0, 2, 0, 2), (2, 0, 3, 0, 0),
        (2, 0, 3, 1, 0), (2, 0, 3, 2, 0), (2, 0, 3, 3, 0),
    ),
)


def norm_rows(tokens, norm_gain):
    values = tokens.astype(jnp.float32)
    scaled = values * lax.rsqrt(jnp.mean(values * values, axis=-1, keepdims=True) + 1e-06)
    return (scaled * norm_gain).astype(jnp.bfloat16)


def expert_hidden(rows, gate_weight, up_weight):
    gate = jnp.einsum("e...d,edf->e...f", rows, gate_weight, preferred_element_type=jnp.float32)
    upper = jnp.einsum("e...d,edf->e...f", rows, up_weight, preferred_element_type=jnp.float32)
    return (jax.nn.silu(gate) * upper).astype(jnp.bfloat16)


def weigh_pieces(summed, weights):
    piece = lax.optimization_barrier(summed.astype(jnp.bfloat16)).astype(jnp.float32)
    total = piece[:, 0] * weights[:, 0:1]
    total = total + piece[:, 1] * weights[:, 1:2]
    return total.astype(jnp.bfloat16)


def plain_body(tokens, norm_gain, gate_weight, up_weight, down_weight, expert_ids, route_weight):
    tok_rows = tokens.shape[0]
    width = tokens.shape[1]
    local_experts = gate_weight.shape[0]
    inner = gate_weight.shape[2]
    n_tp = lax.axis_size("tp")
    n_ep = lax.axis_size("ep")
    experts = n_ep * local_experts
    most = max(2, tok_rows * TOP_K * 5 // (4 * experts))
    normed = norm_rows(tokens, norm_gain)
    flat_ids = expert_ids.reshape(n_tp, tok_rows * TOP_K)
    onehot = (flat_ids[:, :, None] == jnp.arange(experts, dtype=jnp.int32)[None, None, :]).astype(
        jnp.int32
    )
    before = jnp.cumsum(onehot, axis=1) - onehot
    slots = jnp.sum(before * onehot, axis=-1)
    owner = jnp.arange(n_tp, dtype=jnp.int32)[:, None]
    row_index = (flat_ids * (n_tp * most) + owner * most + slots).reshape(-1)
    mine = lax.axis_index("tp")
    own_ids = lax.dynamic_slice_in_dim(flat_ids, mine, 1, 0)[0]
    own_slots = lax.dynamic_slice_in_dim(slots, mine, 1, 0)[0]
    own_index = own_ids * most + own_slots
    whole = lax.all_gather(normed, "tp", axis=0, tiled=True)
    sending = (
        jnp.zeros((experts * n_tp * most, width), jnp.bfloat16)
        .at[row_index]
        .set(jnp.repeat(whole, TOP_K, axis=0))
    )
    arrived = lax.all_to_all(
        sending.reshape(experts, n_tp * most, width), "ep", split_axis=0, concat_axis=1, tiled=True
    )
    hidden = expert_hidden(arrived, gate_weight, up_weight)
    by_source = hidden.reshape(local_experts, n_ep, n_tp, most, inner).transpose(2, 0, 1, 3, 4)
    per_device = local_experts * n_ep * most
    product = jnp.einsum(
        "tlnmf,lfd->tlnmd", by_source, down_weight, preferred_element_type=jnp.float32
    )
    own_sums = lax.psum_scatter(
        product.astype(jnp.bfloat16)
        .astype(jnp.float32)
        .reshape(per_device * lax.axis_size("tp"), width)
        .astype(jnp.bfloat16),
        "tp",
        scatter_dimension=0,
        tiled=True,
    )
    own_pieces = own_sums.reshape(local_experts, n_ep, most, width)
    back = lax.all_to_all(own_pieces, "ep", split_axis=1, concat_axis=0, tiled=True)
    picked = back.reshape(experts * most, width)[own_index].reshape(tok_rows, TOP_K, width)
    own_weights = lax.dynamic_slice_in_dim(route_weight, mine * tok_rows, tok_rows, 0)
    return weigh_pieces(picked.astype(jnp.float32), own_weights)


def neighbour(n, place, edge, piece):
    row, at, number = piece
    if edge == ACROSS:
        return place, (1 - row, at, number), ACROSS
    there = place + (1 if edge == UP else -1)
    return (there, piece, DOWN if edge == UP else UP) if 0 <= there < n else None


def parent(n, crossings, place, piece):
    row, at, number = piece
    goal = at
    if row:
        bits = crossings[at][number]
        places = [k for k in range(n) if bits >> k & 1]
        goal = min(places, key=lambda k: (abs(k - place), abs(k - at)))
    if goal == place:
        return ACROSS if row else None
    return UP if goal > place else DOWN


def children(n, crossings, place, piece):
    found = []
    for edge in (ACROSS, UP, DOWN):
        there = neighbour(n, place, edge, piece)
        if there is not None and parent(n, crossings, there[0], there[1]) == there[2]:
            found.append(edge)
    return found


def choose(index, low, branches):
    if len(branches) == 1:
        branches[0]()
        return
    half = len(branches) // 2
    lax.cond(
        index < low + half,
        lambda: choose(index, low, branches[:half]),
        lambda: choose(index, low + half, branches[half:]),
    )


def pick(index, values):
    result = values[0]
    for i, value in enumerate(values[1:], 1):
        result = jnp.where(index == i, value, result)
    return result


def split(order):
    before, steps, current = [], [], []
    for op in order:
        if op[0] == COMPUTE:
            before.append(current)
            current = []
            if op[4] == 0:
                steps.append(op[1:4])
        else:
            current.append(op)
    return before, steps, current


def kernel(
    n, tok_hbm, gain_hbm, ids_hbm, weight_hbm, gate_hbm, up_hbm, down_hbm, out_ref,
    tok, gain, ids, weight, both, down, hidden, buf, own_shares, shares, part, srecv, rrecv,
    load_sem, w_s, w_r, sib_s, ag_s, rs_s, ag_r, ags_r, rss_r, rs_r,
):
    ep = lax.axis_index("ep")
    z = lax.axis_index("tp")
    y, c = ep // 2, ep % 2
    rows, width = tok.shape
    inner = down.shape[0]
    experts = shares.shape[0]
    per = PIECES // UNITS
    tall = rows // UNITS
    short = rows // PIECES
    sib = {"ep": 2 * y + 1 - c}
    toward = {ACROSS: {"ep": 2 * (1 - y) + c}, UP: {"tp": z + 1}, DOWN: {"tp": z - 1}}

    def row_of(row):
        return row + (1 - 2 * row) * y

    def first(row, at, unit, lane):
        return (((row * n + at) * UNITS + unit) * 2 + lane) * per

    def remote(src, dst, send, recv, to):
        return pltpu.make_async_remote_copy(
            src_ref=src, dst_ref=dst, send_sem=send, recv_sem=recv, device_id=to, device_id_type=MESH
        )

    barrier = pltpu.get_barrier_semaphore()
    for k in range(1, 4):
        pl.semaphore_signal(barrier, inc=1, device_id={"ep": (ep + k) % 4}, device_id_type=MESH)

    @pl.when(z < n - 1)
    def _():
        pl.semaphore_signal(barrier, inc=1, device_id=toward[UP], device_id_type=MESH)

    @pl.when(z > 0)
    def _():
        pl.semaphore_signal(barrier, inc=1, device_id=toward[DOWN], device_id_type=MESH)

    loads = [
        pltpu.make_async_copy(src, dst, load_sem.at[i])
        for i, (src, dst) in enumerate(
            (
                (tok_hbm, tok),
                (gain_hbm, gain),
                (ids_hbm, ids),
                (weight_hbm, weight),
                (gate_hbm.at[0], both.at[:, pl.ds(0, inner)]),
                (up_hbm.at[0], both.at[:, pl.ds(inner, inner)]),
                (down_hbm.at[0], down),
            )
        )
    ]
    for load in loads:
        load.start()

    loads[0].wait()
    loads[1].wait()
    normed = norm_rows(tok[...], gain[...]).reshape(UNITS, per, short, width)
    for unit in range(UNITS):
        buf[pl.ds(first(y, z, unit, c), per)] = normed[unit]
    loads[2].wait()
    loads[3].wait()
    for e in range(experts):
        named = jnp.where(ids[...] == e, weight[...], 0.0)
        total = named[0:1] + named[1:2]
        for k in range(n):
            own_shares[e, k : k + 1, :] = total[:, k * rows : (k + 1) * rows]

    pl.semaphore_wait(barrier, 3 + jnp.where(z > 0, 1, 0) + jnp.where(z < n - 1, 1, 0))

    def share(k):
        to = (ep + k) % 4
        return remote(own_shares.at[to], shares.at[ep], w_s, w_r, {"ep": to})

    def held(yb, at, number, lane):
        return buf.at[first(yb, at, number // per, lane) + number % per]

    def sum_copy(yb, at, unit):
        return remote(part.at[yb, at, unit, 1 - c], srecv.at[yb, at, unit], sib_s, rss_r.at[yb, at, unit], sib)

    def run(here, ops, waited):
        waited = set(waited)
        for op in ops:
            what, row, at, number, edge = op
            yb = row_of(row)
            unit, piece = number // per, number % per
            mine = held(yb, at, number, c)
            own = row == 0 and at == here
            if what == RELAY:
                if not own:
                    remote(mine, mine, ag_s, ag_r.at[yb, at, number], sib).wait_recv()
                remote(mine, mine, sib_s, ags_r.at[yb, at, unit], sib).start()
            elif what == SEND:
                remote(mine, mine, ag_s, ag_r.at[yb, at, number], toward[edge]).start()
            else:
                if (row, at, unit) not in waited:
                    waited.add((row, at, unit))
                    sum_copy(yb, at, unit).wait_recv()
                total = part[yb, at, unit, c, piece].astype(jnp.float32)
                total = total + srecv[yb, at, unit, piece].astype(jnp.float32)
                count = len(children(n, GATHER, here, (row, at, number)))
                if count:
                    landed = rrecv.at[yb, at, number, pl.ds(0, count)]
                    remote(landed, landed, rs_s, rs_r.at[yb, at, number], sib).wait_recv()
                for slot in range(count):
                    total = total + rrecv[yb, at, number, slot].astype(jnp.float32)
                if own:
                    out_ref[number * short : (number + 1) * short, :] = total.astype(out_ref.dtype)
                else:
                    part[yb, at, unit, c, piece] = total.astype(jnp.bfloat16)
                    there, seen_as, back = neighbour(n, here, edge, (row, at, number))
                    slot = children(n, GATHER, there, seen_as).index(back)
                    remote(
                        part.at[yb, at, unit, c, piece], rrecv.at[yb, at, number, slot],
                        rs_s, rs_r.at[yb, at, number], toward[edge],
                    ).start()

    for k in range(1, 4):
        share(k).start()
    shares[ep] = own_shares[ep]

    plans = [split(order) for order in ORDER]
    steps = len(plans[0][1])
    branches, waited = [[] for _ in range(PHASES)], [set() for _ in plans]
    for here, (before, _, _) in enumerate(plans):
        for slot, ops in enumerate(before):
            branches[slot % PHASES].append(functools.partial(run, here, ops, waited[here]))
            waited[here] = waited[here] | {(op[1], op[2], op[3] // per) for op in ops if op[0] == REDUCE}

    def column(row):
        return jnp.transpose(jnp.broadcast_to(row, (rows, rows)))[:, :1]

    lane = lax.broadcasted_iota(jnp.int32, (8, rows), 1)

    def one(step, carry):
        choose(z * steps + step, 0, branches[0])

        @pl.when(step == 0)
        def _():
            for load in loads[4:]:
                load.wait()

        code = pick(z, [pick(step, [(s[0] * n + s[1]) * UNITS + s[2] for s in plan[1]]) for plan in plans])
        row, at, unit = code // (n * UNITS), code // UNITS % n, code % UNITS
        yb = row_of(row)
        theirs = buf.at[pl.ds(first(yb, at, unit, 1 - c), per)]
        remote(theirs, theirs, sib_s, ags_r.at[yb, at, unit], sib).wait_recv()
        x = buf[pl.ds(first(yb, at, unit, 0), 2 * per)].reshape(2 * tall, width)
        mixed = jnp.dot(x, both[...], preferred_element_type=jnp.float32)
        hidden[...] = (jax.nn.silu(mixed[:, :inner]) * mixed[:, inner:]).astype(jnp.bfloat16)
        for later in branches[1:]:
            choose(z * steps + step, 0, later)
        product = jnp.dot(hidden[...], down[...], preferred_element_type=jnp.float32)

        @pl.when(step == 0)
        def _():
            remote(own_shares.at[pl.ds(0, 3)], shares.at[pl.ds(0, 3)], w_s, w_r, sib).wait_recv()

        ours = [jnp.broadcast_to(shares[2 * yb + half, pl.ds(at, 1), :], (8, rows)) for half in range(2)]
        turned = [pltpu.roll(values, tall, 1) for values in ours]
        early = jnp.where(lane < tall, ours[0], turned[1])
        late = jnp.where(lane < tall, turned[0], ours[1])
        w = column(jnp.where(unit == 0, early, late)[0:1])
        part[yb, at, unit] = (product * w).astype(jnp.bfloat16).reshape(2, per, short, width)
        sum_copy(yb, at, unit).start()
        return carry

    lax.fori_loop(0, steps, one, 0)

    def finish(here):
        run(here, plans[here][2], waited[here])
        for what, sem in ((SEND, ag_s), (REDUCE, rs_s)):
            count = sum(op[0] == what and (what == SEND or op[1] > 0 or op[2] != here) for op in ORDER[here])
            sent = buf.at[pl.ds(0, count)]
            remote(sent, sent, sem, sem, sib).wait_send()

    choose(z, 0, [functools.partial(finish, here) for here in range(len(plans))])
    remote(buf, buf, sib_s, sib_s, sib).wait_send()
    remote(own_shares.at[pl.ds(0, 3)], shares.at[pl.ds(0, 3)], w_s, w_r, sib).wait_send()


def kernel_bytes(n, rows, width, inner):
    blocks = n * 4 + 2 * n * 2 + 2 * n + 6 * n + 4
    return 2 * width * (3 * inner + blocks * rows) + 16 * rows * (width + 2 * inner)


def fused_body(tokens, norm_gain, gate_weight, up_weight, down_weight, expert_ids, route_weight):
    rows, width = tokens.shape
    inner = gate_weight.shape[2]
    n = lax.axis_size("tp")
    experts = lax.axis_size("ep")
    vmem = pl.BlockSpec(memory_space=pltpu.VMEM)
    anywhere = pl.BlockSpec(memory_space=pl.ANY)
    dma = pltpu.SemaphoreType.DMA
    bf16 = jnp.bfloat16
    per, short = PIECES // UNITS, rows // PIECES
    return pl.pallas_call(
        functools.partial(kernel, n),
        out_shape=jax.ShapeDtypeStruct((rows, width), bf16),
        in_specs=[anywhere] * 7,
        out_specs=vmem,
        scratch_shapes=[
            pltpu.VMEM((rows, width), bf16),
            pltpu.VMEM((1, width), jnp.float32),
            pltpu.VMEM((TOP_K, n * rows), jnp.int32),
            pltpu.VMEM((TOP_K, n * rows), jnp.float32),
            pltpu.VMEM((width, 2 * inner), bf16),
            pltpu.VMEM((inner, width), bf16),
            pltpu.VMEM((2 * rows // UNITS, inner), bf16),
            pltpu.VMEM((2 * n * UNITS * 2 * per, short, width), bf16),
            pltpu.VMEM((experts, n, rows), jnp.float32),
            pltpu.VMEM((experts, n, rows), jnp.float32),
            pltpu.VMEM((2, n, UNITS, 2, per, short, width), bf16),
            pltpu.VMEM((2, n, UNITS, per, short, width), bf16),
            pltpu.VMEM((2, n, PIECES, 3, short, width), bf16),
            dma((7,)),
            dma,
            dma,
            dma,
            dma,
            dma,
            dma((2, n, PIECES)),
            dma((2, n, UNITS)),
            dma((2, n, UNITS)),
            dma((2, n, PIECES)),
        ],
        compiler_params=pltpu.CompilerParams(
            collective_id=0, has_side_effects=True, vmem_limit_bytes=VMEM_ROOM
        ),
    )(tokens, norm_gain.reshape(1, width), expert_ids.T, route_weight.T, gate_weight, up_weight, down_weight)


def body(tokens, norm_gain, gate_weight, up_weight, down_weight, expert_ids, route_weight):
    rows, width = tokens.shape
    inner = gate_weight.shape[2]
    n = lax.axis_size("tp")
    fits = kernel_bytes(n, rows, width, inner) <= VMEM_ROOM and rows % 128 == 0
    chosen = plain_body
    if lax.axis_size("ep") == 4 and gate_weight.shape[0] == 1 and n == LINE and fits:
        chosen = fused_body
    return chosen(tokens, norm_gain, gate_weight, up_weight, down_weight, expert_ids, route_weight)


def solution(mesh):
    placed = (
        P(("grp", "ep", "tp"), None),
        P(),
        P("ep", None, "tp"),
        P("ep", None, "tp"),
        P("ep", "tp", None),
        P(("grp", "ep"), None),
        P(("grp", "ep"), None),
    )
    return jax.shard_map(
        body, mesh=mesh, in_specs=placed, out_specs=P(("grp", "ep", "tp"), None), check_vma=False
    )
```

```python
import functools

import jax
import jax.numpy as jnp
from jax import lax
from jax.experimental import pallas as pl
from jax.experimental.pallas import tpu as pltpu
from jax.sharding import PartitionSpec as P

TOP_K = 2
MESH = pl.DeviceIdType.MESH
VMEM_ROOM = 60 << 20

ACROSS, UP, DOWN = range(3)
RELAY, SEND, REDUCE, COMPUTE = range(4)
UNITS = 2
PIECES = 4
PHASES = 1
LINE = 4
SPREAD = ((15, 5, 13, 11), (1, 3, 7, 15), (7, 7, 13, 14), (10, 12, 11, 10))
GATHER = ((1, 11, 13, 1), (8, 14, 12, 15), (8, 15, 7, 11), (8, 7, 13, 11))
ORDER = (
    (
        (0, 0, 0, 0, 0), (0, 0, 0, 1, 0), (0, 0, 0, 2, 0), (0, 0, 0, 3, 0), (1, 0, 0, 1, 1), (1, 0, 0, 1, 0),
        (1, 0, 0, 0, 1), (1, 0, 0, 0, 0), (3, 0, 0, 0, 0), (1, 0, 0, 2, 1), (1, 0, 0, 3, 0), (3, 0, 0, 1, 0),
        (1, 0, 0, 3, 1), (1, 0, 0, 2, 0), (0, 1, 0, 1, 0), (0, 0, 1, 0, 0), (1, 1, 0, 1, 1), (1, 0, 1, 0, 0),
        (0, 1, 0, 0, 0), (0, 0, 1, 1, 0), (3, 1, 0, 0, 0), (0, 1, 0, 3, 0), (1, 0, 1, 1, 0), (3, 0, 1, 0, 0),
        (0, 0, 1, 2, 0), (0, 1, 0, 2, 0), (1, 1, 0, 2, 1), (1, 0, 1, 2, 0), (0, 0, 1, 3, 0), (1, 0, 1, 3, 0),
        (0, 1, 1, 0, 0), (1, 1, 1, 0, 1), (3, 1, 0, 1, 0), (0, 0, 2, 1, 0), (0, 1, 1, 1, 0), (2, 0, 1, 0, 1),
        (2, 1, 0, 1, 0), (3, 0, 1, 1, 0), (0, 0, 2, 0, 0), (0, 1, 1, 2, 0), (2, 0, 1, 1, 1), (1, 0, 2, 1, 0),
        (3, 1, 1, 0, 0), (0, 0, 3, 0, 0), (2, 0, 1, 2, 1), (0, 1, 1, 3, 0), (1, 0, 2, 0, 0), (3, 0, 2, 0, 0),
        (0, 0, 2, 2, 0), (2, 1, 1, 0, 1), (1, 0, 2, 2, 0), (3, 1, 1, 1, 0), (0, 0, 3, 2, 0), (2, 0, 2, 0, 1),
        (1, 0, 3, 2, 0), (0, 1, 2, 1, 0), (0, 1, 3, 0, 0), (2, 1, 1, 1, 1), (2, 1, 1, 3, 0), (0, 1, 2, 0, 0),
        (0, 1, 3, 1, 0), (2, 1, 1, 2, 1), (3, 1, 2, 0, 0), (0, 1, 2, 2, 0), (3, 1, 3, 0, 0), (0, 0, 3, 1, 0),
        (0, 1, 3, 2, 0), (2, 1, 2, 0, 1), (2, 1, 2, 1, 0), (0, 1, 3, 3, 0), (2, 0, 1, 3, 1), (3, 0, 3, 0, 0),
        (0, 0, 3, 3, 0), (2, 1, 3, 1, 0), (2, 1, 3, 0, 1), (3, 1, 3, 1, 0), (0, 0, 2, 3, 0), (2, 0, 2, 1, 1),
        (3, 0, 3, 1, 0), (0, 1, 2, 3, 0), (2, 1, 3, 3, 0), (2, 0, 3, 0, 1), (3, 0, 2, 1, 0), (2, 1, 3, 2, 0),
        (2, 0, 3, 1, 1), (3, 1, 2, 1, 0), (2, 1, 0, 2, 0), (2, 0, 3, 3, 1), (2, 1, 2, 2, 0), (2, 1, 2, 3, 0),
        (2, 0, 3, 2, 1), (2, 0, 2, 2, 1), (2, 1, 0, 0, 0), (2, 0, 2, 3, 1), (2, 1, 0, 3, 0), (2, 0, 0, 1, 0),
        (2, 0, 0, 0, 0), (2, 0, 0, 2, 0), (2, 0, 0, 3, 0),
    ),
    (
        (0, 0, 1, 0, 0), (0, 0, 1, 1, 0), (0, 0, 1, 2, 0), (0, 0, 1, 3, 0), (1, 0, 1, 1, 0), (1, 0, 1, 0, 2),
        (1, 0, 1, 3, 1), (1, 0, 1, 2, 0), (1, 0, 1, 1, 2), (1, 0, 1, 1, 1), (3, 0, 1, 0, 0), (1, 0, 1, 2, 2),
        (1, 0, 1, 0, 1), (1, 0, 1, 3, 0), (3, 0, 1, 1, 0), (0, 0, 0, 1, 0), (0, 1, 1, 1, 0), (1, 0, 0, 1, 1),
        (1, 0, 1, 3, 2), (0, 0, 2, 1, 0), (1, 0, 2, 1, 0), (0, 0, 0, 0, 0), (1, 0, 0, 0, 0), (0, 1, 1, 2, 0),
        (1, 0, 2, 1, 2), (1, 0, 0, 0, 1), (3, 0, 0, 0, 0), (0, 0, 0, 2, 0), (0, 0, 2, 0, 0), (1, 0, 2, 0, 0),
        (0, 1, 1, 3, 0), (1, 0, 2, 0, 2), (1, 0, 0, 2, 1), (0, 0, 2, 2, 0), (0, 0, 0, 3, 0), (3, 0, 2, 0, 0),
        (0, 0, 3, 0, 0), (0, 1, 0, 1, 0), (0, 1, 2, 1, 0), (1, 0, 3, 0, 0), (1, 0, 3, 0, 2), (1, 0, 0, 3, 1),
        (3, 1, 1, 1, 0), (0, 1, 0, 0, 0), (0, 1, 2, 2, 0), (1, 0, 2, 2, 2), (1, 0, 1, 2, 1), (1, 0, 0, 3, 0),
        (3, 0, 0, 1, 0), (0, 0, 3, 2, 0), (0, 1, 0, 2, 0), (0, 1, 2, 0, 0), (1, 0, 3, 2, 0), (1, 1, 1, 1, 1),
        (1, 0, 3, 2, 2), (3, 1, 0, 0, 0), (0, 0, 3, 3, 0), (0, 1, 1, 0, 0), (0, 1, 3, 0, 0), (1, 1, 3, 0, 2),
        (1, 1, 1, 0, 1), (1, 0, 3, 3, 0), (3, 1, 2, 0, 0), (0, 1, 0, 3, 0), (0, 1, 3, 1, 0), (1, 1, 0, 3, 1),
        (1, 1, 3, 1, 2), (2, 1, 1, 3, 0), (3, 0, 3, 1, 0), (0, 0, 3, 1, 0), (0, 1, 3, 2, 0), (1, 0, 3, 1, 2),
        (2, 1, 2, 1, 0), (3, 1, 3, 0, 0), (0, 0, 2, 3, 0), (0, 1, 3, 3, 0), (1, 1, 3, 3, 2), (1, 0, 2, 3, 0),
        (3, 1, 1, 0, 0), (2, 1, 3, 1, 0), (1, 0, 3, 3, 2), (3, 1, 3, 1, 0), (2, 1, 1, 0, 1), (1, 0, 2, 3, 2),
        (3, 0, 2, 1, 0), (2, 1, 3, 3, 0), (2, 0, 2, 0, 1), (0, 1, 2, 3, 0), (1, 1, 2, 3, 2), (3, 1, 0, 1, 0),
        (2, 1, 1, 1, 0), (2, 1, 3, 2, 1), (3, 1, 2, 1, 0), (2, 1, 1, 2, 1), (2, 1, 0, 2, 2), (3, 0, 3, 0, 0),
        (2, 1, 2, 3, 0), (2, 1, 2, 0, 1), (2, 1, 2, 2, 0), (2, 0, 0, 0, 2), (2, 1, 0, 1, 0), (2, 1, 3, 0, 1),
        (2, 0, 2, 1, 1), (2, 0, 0, 3, 2), (2, 0, 3, 0, 1), (2, 1, 0, 0, 2), (2, 0, 3, 1, 1), (2, 1, 0, 3, 2),
        (2, 0, 3, 3, 1), (2, 0, 0, 1, 2), (2, 0, 3, 2, 1), (2, 0, 0, 2, 2), (2, 0, 1, 1, 0), (2, 0, 2, 2, 1),
        (2, 0, 1, 2, 0), (2, 0, 2, 3, 1), (2, 0, 1, 3, 0), (2, 0, 1, 0, 0),
    ),
    (
        (0, 0, 2, 0, 0), (0, 0, 2, 1, 0), (0, 0, 2, 2, 0), (0, 0, 2, 3, 0), (1, 0, 2, 1, 2), (1, 0, 2, 2, 1),
        (1, 0, 2, 2, 0), (1, 0, 2, 0, 2), (1, 0, 2, 3, 1), (1, 0, 2, 3, 0), (3, 0, 2, 0, 0), (1, 0, 2, 2, 2),
        (1, 0, 2, 1, 1), (1, 0, 2, 0, 0), (3, 0, 2, 1, 0), (0, 0, 3, 0, 0), (0, 0, 1, 3, 0), (0, 1, 2, 2, 0),
        (1, 0, 3, 0, 2), (1, 0, 1, 3, 0), (1, 0, 1, 3, 1), (0, 0, 1, 1, 0), (1, 1, 2, 2, 2), (0, 0, 3, 1, 0),
        (1, 0, 3, 1, 0), (0, 1, 2, 3, 0), (1, 0, 1, 1, 1), (3, 0, 3, 0, 0), (0, 0, 3, 2, 0), (0, 0, 1, 0, 0),
        (0, 1, 2, 0, 0), (1, 0, 3, 2, 2), (1, 0, 1, 0, 1), (1, 0, 2, 1, 0), (3, 1, 2, 1, 0), (0, 0, 3, 3, 0),
        (0, 0, 0, 1, 0), (0, 1, 1, 3, 0), (1, 0, 0, 1, 0), (1, 0, 3, 3, 2), (1, 0, 0, 1, 1), (3, 0, 1, 0, 0),
        (0, 0, 0, 0, 0), (0, 1, 3, 1, 0), (0, 1, 3, 2, 0), (1, 0, 0, 0, 0), (1, 1, 3, 1, 2), (1, 0, 0, 0, 1),
        (3, 0, 3, 1, 0), (0, 0, 0, 2, 0), (0, 1, 2, 1, 0), (0, 1, 3, 3, 0), (1, 0, 0, 2, 1), (1, 0, 0, 2, 0),
        (1, 0, 3, 1, 2), (3, 0, 0, 0, 0), (0, 0, 0, 3, 0), (0, 1, 0, 1, 0), (0, 1, 3, 0, 0), (1, 0, 0, 3, 1),
        (1, 0, 2, 3, 2), (3, 1, 3, 1, 0), (0, 0, 1, 2, 0), (0, 1, 0, 0, 0), (1, 0, 1, 2, 0), (1, 1, 0, 1, 1),
        (2, 1, 2, 3, 2), (3, 1, 2, 0, 0), (0, 1, 1, 1, 0), (0, 1, 0, 2, 0), (1, 1, 1, 1, 1), (3, 0, 1, 1, 0),
        (0, 1, 1, 0, 0), (2, 1, 2, 1, 0), (1, 1, 1, 0, 1), (3, 1, 0, 0, 0), (0, 1, 1, 2, 0), (0, 1, 0, 3, 0),
        (1, 1, 1, 2, 1), (3, 0, 0, 1, 0), (3, 1, 3, 0, 0), (2, 1, 0, 1, 2), (1, 0, 1, 2, 1), (2, 1, 2, 2, 0),
        (3, 1, 1, 1, 0), (2, 1, 3, 1, 0), (1, 1, 2, 1, 1), (2, 0, 0, 0, 2), (3, 1, 1, 0, 0), (2, 1, 1, 3, 0),
        (1, 1, 2, 0, 1), (3, 1, 0, 1, 0), (2, 1, 1, 1, 0), (2, 1, 1, 0, 1), (2, 0, 0, 3, 2), (2, 1, 3, 3, 1),
        (2, 1, 0, 0, 2), (2, 1, 3, 2, 0), (1, 0, 2, 0, 1), (2, 1, 0, 2, 0), (2, 1, 0, 3, 2), (2, 1, 1, 2, 0),
        (2, 1, 2, 0, 1), (2, 0, 0, 1, 2), (2, 1, 3, 0, 1), (2, 0, 0, 2, 2), (2, 0, 1, 1, 2), (2, 0, 3, 0, 1),
        (2, 0, 1, 2, 2), (2, 0, 3, 1, 1), (2, 0, 1, 3, 2), (2, 0, 3, 3, 1), (2, 0, 1, 0, 2), (2, 0, 3, 2, 1),
        (2, 0, 2, 1, 0), (2, 0, 2, 2, 0), (2, 0, 2, 0, 0), (2, 0, 2, 3, 0),
    ),
    (
        (0, 0, 3, 0, 0), (0, 0, 3, 1, 0), (0, 0, 3, 2, 0), (0, 0, 3, 3, 0), (1, 0, 3, 0, 2), (1, 0, 3, 2, 0),
        (1, 0, 3, 1, 2), (1, 0, 3, 1, 0), (3, 0, 3, 0, 0), (1, 0, 3, 3, 0), (1, 0, 3, 2, 2), (3, 0, 3, 1, 0),
        (1, 0, 3, 3, 2), (1, 0, 3, 0, 0), (0, 0, 2, 2, 0), (0, 1, 3, 2, 0), (1, 1, 3, 2, 2), (1, 0, 2, 2, 0),
        (0, 0, 2, 3, 0), (0, 1, 3, 1, 0), (3, 0, 2, 1, 0), (0, 1, 3, 3, 0), (0, 0, 2, 1, 0), (1, 0, 2, 3, 0),
        (1, 1, 3, 3, 2), (0, 0, 1, 3, 0), (0, 1, 3, 0, 0), (1, 0, 1, 3, 0), (1, 1, 3, 0, 2), (3, 1, 3, 1, 0),
        (0, 0, 1, 1, 0), (0, 1, 2, 2, 0), (2, 0, 2, 2, 2), (3, 1, 3, 0, 0), (0, 0, 1, 0, 0), (0, 1, 2, 3, 0),
        (2, 1, 3, 2, 0), (3, 0, 1, 0, 0), (0, 0, 0, 1, 0), (0, 1, 1, 3, 0), (2, 1, 3, 1, 2), (3, 1, 2, 1, 0),
        (0, 0, 0, 0, 0), (1, 0, 0, 0, 0), (0, 0, 0, 2, 0), (1, 0, 0, 2, 0), (3, 0, 0, 0, 0), (0, 0, 0, 3, 0),
        (1, 0, 0, 3, 0), (2, 1, 2, 2, 2), (2, 1, 2, 3, 0), (0, 1, 0, 0, 0), (2, 0, 0, 0, 2), (0, 1, 0, 1, 0),
        (3, 0, 0, 1, 0), (3, 1, 0, 0, 0), (0, 1, 0, 2, 0), (0, 1, 1, 1, 0), (2, 0, 0, 3, 2), (0, 1, 0, 3, 0),
        (0, 1, 1, 0, 0), (2, 1, 0, 0, 2), (2, 1, 0, 1, 0), (3, 1, 0, 1, 0), (0, 1, 1, 2, 0), (2, 0, 2, 3, 2),
        (3, 1, 1, 0, 0), (0, 0, 1, 2, 0), (2, 1, 0, 2, 0), (2, 1, 0, 3, 2), (3, 1, 1, 1, 0), (0, 1, 2, 1, 0),
        (2, 1, 1, 1, 0), (2, 0, 0, 1, 2), (3, 0, 1, 1, 0), (0, 1, 2, 0, 0), (2, 1, 1, 2, 0), (2, 1, 1, 3, 0),
        (2, 0, 0, 2, 2), (3, 1, 2, 0, 0), (2, 0, 1, 1, 2), (2, 1, 1, 0, 0), (2, 1, 3, 3, 0), (2, 0, 1, 2, 2),
        (0, 0, 2, 0, 0), (2, 1, 2, 1, 0), (2, 0, 1, 3, 2), (3, 0, 2, 0, 0), (2, 1, 2, 0, 0), (2, 0, 1, 0, 2),
        (2, 1, 3, 0, 0), (2, 0, 2, 1, 2), (2, 0, 2, 0, 2), (2, 0, 3, 1, 0), (2, 0, 3, 0, 0), (2, 0, 3, 3, 0),
        (2, 0, 3, 2, 0),
    ),
)


def norm_rows(tokens, norm_gain):
    values = tokens.astype(jnp.float32)
    scaled = values * lax.rsqrt(jnp.mean(values * values, axis=-1, keepdims=True) + 1e-06)
    return (scaled * norm_gain).astype(jnp.bfloat16)


def expert_hidden(rows, gate_weight, up_weight):
    gate = jnp.einsum("e...d,edf->e...f", rows, gate_weight, preferred_element_type=jnp.float32)
    upper = jnp.einsum("e...d,edf->e...f", rows, up_weight, preferred_element_type=jnp.float32)
    return (jax.nn.silu(gate) * upper).astype(jnp.bfloat16)


def weigh_pieces(summed, weights):
    piece = lax.optimization_barrier(summed.astype(jnp.bfloat16)).astype(jnp.float32)
    total = piece[:, 0] * weights[:, 0:1]
    total = total + piece[:, 1] * weights[:, 1:2]
    return total.astype(jnp.bfloat16)


def plain_body(tokens, norm_gain, gate_weight, up_weight, down_weight, expert_ids, route_weight):
    tok_rows = tokens.shape[0]
    width = tokens.shape[1]
    local_experts = gate_weight.shape[0]
    inner = gate_weight.shape[2]
    n_tp = lax.axis_size("tp")
    n_ep = lax.axis_size("ep")
    experts = n_ep * local_experts
    most = max(2, tok_rows * TOP_K * 5 // (4 * experts))
    normed = norm_rows(tokens, norm_gain)
    flat_ids = expert_ids.reshape(n_tp, tok_rows * TOP_K)
    onehot = (flat_ids[:, :, None] == jnp.arange(experts, dtype=jnp.int32)[None, None, :]).astype(
        jnp.int32
    )
    before = jnp.cumsum(onehot, axis=1) - onehot
    slots = jnp.sum(before * onehot, axis=-1)
    owner = jnp.arange(n_tp, dtype=jnp.int32)[:, None]
    row_index = (flat_ids * (n_tp * most) + owner * most + slots).reshape(-1)
    mine = lax.axis_index("tp")
    own_ids = lax.dynamic_slice_in_dim(flat_ids, mine, 1, 0)[0]
    own_slots = lax.dynamic_slice_in_dim(slots, mine, 1, 0)[0]
    own_index = own_ids * most + own_slots
    whole = lax.all_gather(normed, "tp", axis=0, tiled=True)
    sending = (
        jnp.zeros((experts * n_tp * most, width), jnp.bfloat16)
        .at[row_index]
        .set(jnp.repeat(whole, TOP_K, axis=0))
    )
    arrived = lax.all_to_all(
        sending.reshape(experts, n_tp * most, width), "ep", split_axis=0, concat_axis=1, tiled=True
    )
    hidden = expert_hidden(arrived, gate_weight, up_weight)
    by_source = hidden.reshape(local_experts, n_ep, n_tp, most, inner).transpose(2, 0, 1, 3, 4)
    per_device = local_experts * n_ep * most
    product = jnp.einsum(
        "tlnmf,lfd->tlnmd", by_source, down_weight, preferred_element_type=jnp.float32
    )
    own_sums = lax.psum_scatter(
        product.astype(jnp.bfloat16)
        .astype(jnp.float32)
        .reshape(per_device * lax.axis_size("tp"), width)
        .astype(jnp.bfloat16),
        "tp",
        scatter_dimension=0,
        tiled=True,
    )
    own_pieces = own_sums.reshape(local_experts, n_ep, most, width)
    back = lax.all_to_all(own_pieces, "ep", split_axis=1, concat_axis=0, tiled=True)
    picked = back.reshape(experts * most, width)[own_index].reshape(tok_rows, TOP_K, width)
    own_weights = lax.dynamic_slice_in_dim(route_weight, mine * tok_rows, tok_rows, 0)
    return weigh_pieces(picked.astype(jnp.float32), own_weights)


def neighbour(n, place, edge, piece):
    row, at, number = piece
    if edge == ACROSS:
        return place, (1 - row, at, number), ACROSS
    there = place + (1 if edge == UP else -1)
    return (there, piece, DOWN if edge == UP else UP) if 0 <= there < n else None


def parent(n, crossings, place, piece):
    row, at, number = piece
    goal = at
    if row:
        bits = crossings[at][number]
        places = [k for k in range(n) if bits >> k & 1]
        goal = min(places, key=lambda k: (abs(k - place), abs(k - at)))
    if goal == place:
        return ACROSS if row else None
    return UP if goal > place else DOWN


def children(n, crossings, place, piece):
    found = []
    for edge in (ACROSS, UP, DOWN):
        there = neighbour(n, place, edge, piece)
        if there is not None and parent(n, crossings, there[0], there[1]) == there[2]:
            found.append(edge)
    return found


def choose(index, low, branches):
    if len(branches) == 1:
        branches[0]()
        return
    half = len(branches) // 2
    lax.cond(
        index < low + half,
        lambda: choose(index, low, branches[:half]),
        lambda: choose(index, low + half, branches[half:]),
    )


def pick(index, values):
    result = values[0]
    for i, value in enumerate(values[1:], 1):
        result = jnp.where(index == i, value, result)
    return result


def split(order):
    before, steps, current = [], [], []
    for op in order:
        if op[0] == COMPUTE:
            before.append(current)
            current = []
            if op[4] == 0:
                steps.append(op[1:4])
        else:
            current.append(op)
    return before, steps, current


def kernel(
    n, tok_hbm, gain_hbm, ids_hbm, weight_hbm, gate_hbm, up_hbm, down_hbm, out_ref,
    tok, gain, ids, weight, both, down, hidden, buf, own_shares, shares, part, srecv, rrecv,
    load_sem, w_s, w_r, sib_s, ag_s, rs_s, ag_r, ags_r, rss_r, rs_r,
):
    ep = lax.axis_index("ep")
    z = lax.axis_index("tp")
    y, c = ep // 2, ep % 2
    rows, width = tok.shape
    inner = down.shape[0]
    experts = shares.shape[0]
    per = PIECES // UNITS
    tall = rows // UNITS
    short = rows // PIECES
    sib = {"ep": 2 * y + 1 - c}
    toward = {ACROSS: {"ep": 2 * (1 - y) + c}, UP: {"tp": z + 1}, DOWN: {"tp": z - 1}}

    def row_of(row):
        return row + (1 - 2 * row) * y

    def first(row, at, unit, lane):
        return (((row * n + at) * UNITS + unit) * 2 + lane) * per

    def remote(src, dst, send, recv, to):
        return pltpu.make_async_remote_copy(
            src_ref=src, dst_ref=dst, send_sem=send, recv_sem=recv, device_id=to, device_id_type=MESH
        )

    barrier = pltpu.get_barrier_semaphore()
    for k in range(1, 4):
        pl.semaphore_signal(barrier, inc=1, device_id={"ep": (ep + k) % 4}, device_id_type=MESH)

    @pl.when(z < n - 1)
    def _():
        pl.semaphore_signal(barrier, inc=1, device_id=toward[UP], device_id_type=MESH)

    @pl.when(z > 0)
    def _():
        pl.semaphore_signal(barrier, inc=1, device_id=toward[DOWN], device_id_type=MESH)

    loads = [
        pltpu.make_async_copy(src, dst, load_sem.at[i])
        for i, (src, dst) in enumerate(
            (
                (tok_hbm, tok),
                (gain_hbm, gain),
                (ids_hbm, ids),
                (weight_hbm, weight),
                (gate_hbm.at[0], both.at[:, pl.ds(0, inner)]),
                (up_hbm.at[0], both.at[:, pl.ds(inner, inner)]),
                (down_hbm.at[0], down),
            )
        )
    ]
    for load in loads:
        load.start()

    loads[0].wait()
    loads[1].wait()
    normed = norm_rows(tok[...], gain[...]).reshape(UNITS, per, short, width)
    for unit in range(UNITS):
        buf[pl.ds(first(y, z, unit, c), per)] = normed[unit]
    loads[2].wait()
    loads[3].wait()
    for e in range(experts):
        named = jnp.where(ids[...] == e, weight[...], 0.0)
        total = named[0:1] + named[1:2]
        for k in range(n):
            own_shares[e, k : k + 1, :] = total[:, k * rows : (k + 1) * rows]

    pl.semaphore_wait(barrier, 3 + jnp.where(z > 0, 1, 0) + jnp.where(z < n - 1, 1, 0))

    def share(k):
        to = (ep + k) % 4
        return remote(own_shares.at[to], shares.at[ep], w_s, w_r, {"ep": to})

    def held(yb, at, number, lane):
        return buf.at[first(yb, at, number // per, lane) + number % per]

    def sum_copy(yb, at, unit):
        return remote(part.at[yb, at, unit, 1 - c], srecv.at[yb, at, unit], sib_s, rss_r.at[yb, at, unit], sib)

    def run(here, ops, waited):
        waited = set(waited)
        for op in ops:
            what, row, at, number, edge = op
            yb = row_of(row)
            unit, piece = number // per, number % per
            mine = held(yb, at, number, c)
            own = row == 0 and at == here
            if what == RELAY:
                if not own:
                    remote(mine, mine, ag_s, ag_r.at[yb, at, number], sib).wait_recv()
                remote(mine, mine, sib_s, ags_r.at[yb, at, unit], sib).start()
            elif what == SEND:
                remote(mine, mine, ag_s, ag_r.at[yb, at, number], toward[edge]).start()
            else:
                if (row, at, unit) not in waited:
                    waited.add((row, at, unit))
                    sum_copy(yb, at, unit).wait_recv()
                total = part[yb, at, unit, c, piece].astype(jnp.float32)
                total = total + srecv[yb, at, unit, piece].astype(jnp.float32)
                count = len(children(n, GATHER, here, (row, at, number)))
                if count:
                    landed = rrecv.at[yb, at, number, pl.ds(0, count)]
                    remote(landed, landed, rs_s, rs_r.at[yb, at, number], sib).wait_recv()
                for slot in range(count):
                    total = total + rrecv[yb, at, number, slot].astype(jnp.float32)
                if own:
                    out_ref[number * short : (number + 1) * short, :] = total.astype(out_ref.dtype)
                else:
                    part[yb, at, unit, c, piece] = total.astype(jnp.bfloat16)
                    there, seen_as, back = neighbour(n, here, edge, (row, at, number))
                    slot = children(n, GATHER, there, seen_as).index(back)
                    remote(
                        part.at[yb, at, unit, c, piece], rrecv.at[yb, at, number, slot],
                        rs_s, rs_r.at[yb, at, number], toward[edge],
                    ).start()

    for k in range(1, 4):
        share(k).start()
    shares[ep] = own_shares[ep]

    plans = [split(order) for order in ORDER]
    steps = len(plans[0][1])
    branches, waited = [[] for _ in range(PHASES)], [set() for _ in plans]
    for here, (before, _, _) in enumerate(plans):
        for slot, ops in enumerate(before):
            branches[slot % PHASES].append(functools.partial(run, here, ops, waited[here]))
            waited[here] = waited[here] | {(op[1], op[2], op[3] // per) for op in ops if op[0] == REDUCE}

    def column(row):
        return jnp.transpose(jnp.broadcast_to(row, (rows, rows)))[:, :1]

    lane = lax.broadcasted_iota(jnp.int32, (8, rows), 1)

    def one(step, carry):
        choose(z * steps + step, 0, branches[0])

        @pl.when(step == 0)
        def _():
            for load in loads[4:]:
                load.wait()

        code = pick(z, [pick(step, [(s[0] * n + s[1]) * UNITS + s[2] for s in plan[1]]) for plan in plans])
        row, at, unit = code // (n * UNITS), code // UNITS % n, code % UNITS
        yb = row_of(row)
        theirs = buf.at[pl.ds(first(yb, at, unit, 1 - c), per)]
        remote(theirs, theirs, sib_s, ags_r.at[yb, at, unit], sib).wait_recv()
        x = buf[pl.ds(first(yb, at, unit, 0), 2 * per)].reshape(2 * tall, width)
        mixed = jnp.dot(x, both[...], preferred_element_type=jnp.float32)
        hidden[...] = (jax.nn.silu(mixed[:, :inner]) * mixed[:, inner:]).astype(jnp.bfloat16)
        for later in branches[1:]:
            choose(z * steps + step, 0, later)
        product = jnp.dot(hidden[...], down[...], preferred_element_type=jnp.float32)

        @pl.when(step == 0)
        def _():
            remote(own_shares.at[pl.ds(0, 3)], shares.at[pl.ds(0, 3)], w_s, w_r, sib).wait_recv()

        ours = [jnp.broadcast_to(shares[2 * yb + half, pl.ds(at, 1), :], (8, rows)) for half in range(2)]
        turned = [pltpu.roll(values, tall, 1) for values in ours]
        early = jnp.where(lane < tall, ours[0], turned[1])
        late = jnp.where(lane < tall, turned[0], ours[1])
        w = column(jnp.where(unit == 0, early, late)[0:1])
        part[yb, at, unit] = (product * w).astype(jnp.bfloat16).reshape(2, per, short, width)
        sum_copy(yb, at, unit).start()
        return carry

    lax.fori_loop(0, steps, one, 0)

    def finish(here):
        run(here, plans[here][2], waited[here])
        for what, sem in ((SEND, ag_s), (REDUCE, rs_s)):
            count = sum(op[0] == what and (what == SEND or op[1] > 0 or op[2] != here) for op in ORDER[here])
            sent = buf.at[pl.ds(0, count)]
            remote(sent, sent, sem, sem, sib).wait_send()

    choose(z, 0, [functools.partial(finish, here) for here in range(len(plans))])
    remote(buf, buf, sib_s, sib_s, sib).wait_send()
    remote(own_shares.at[pl.ds(0, 3)], shares.at[pl.ds(0, 3)], w_s, w_r, sib).wait_send()


def kernel_bytes(n, rows, width, inner):
    blocks = n * 4 + 2 * n * 2 + 2 * n + 6 * n + 4
    return 2 * width * (3 * inner + blocks * rows) + 16 * rows * (width + 2 * inner)


def fused_body(tokens, norm_gain, gate_weight, up_weight, down_weight, expert_ids, route_weight):
    rows, width = tokens.shape
    inner = gate_weight.shape[2]
    n = lax.axis_size("tp")
    experts = lax.axis_size("ep")
    vmem = pl.BlockSpec(memory_space=pltpu.VMEM)
    anywhere = pl.BlockSpec(memory_space=pl.ANY)
    dma = pltpu.SemaphoreType.DMA
    bf16 = jnp.bfloat16
    per, short = PIECES // UNITS, rows // PIECES
    return pl.pallas_call(
        functools.partial(kernel, n),
        out_shape=jax.ShapeDtypeStruct((rows, width), bf16),
        in_specs=[anywhere] * 7,
        out_specs=vmem,
        scratch_shapes=[
            pltpu.VMEM((rows, width), bf16),
            pltpu.VMEM((1, width), jnp.float32),
            pltpu.VMEM((TOP_K, n * rows), jnp.int32),
            pltpu.VMEM((TOP_K, n * rows), jnp.float32),
            pltpu.VMEM((width, 2 * inner), bf16),
            pltpu.VMEM((inner, width), bf16),
            pltpu.VMEM((2 * rows // UNITS, inner), bf16),
            pltpu.VMEM((2 * n * UNITS * 2 * per, short, width), bf16),
            pltpu.VMEM((experts, n, rows), jnp.float32),
            pltpu.VMEM((experts, n, rows), jnp.float32),
            pltpu.VMEM((2, n, UNITS, 2, per, short, width), bf16),
            pltpu.VMEM((2, n, UNITS, per, short, width), bf16),
            pltpu.VMEM((2, n, PIECES, 3, short, width), bf16),
            dma((7,)),
            dma,
            dma,
            dma,
            dma,
            dma,
            dma((2, n, PIECES)),
            dma((2, n, UNITS)),
            dma((2, n, UNITS)),
            dma((2, n, PIECES)),
        ],
        compiler_params=pltpu.CompilerParams(
            collective_id=0, has_side_effects=True, vmem_limit_bytes=VMEM_ROOM
        ),
    )(tokens, norm_gain.reshape(1, width), expert_ids.T, route_weight.T, gate_weight, up_weight, down_weight)


def body(tokens, norm_gain, gate_weight, up_weight, down_weight, expert_ids, route_weight):
    rows, width = tokens.shape
    inner = gate_weight.shape[2]
    n = lax.axis_size("tp")
    fits = kernel_bytes(n, rows, width, inner) <= VMEM_ROOM and rows % 128 == 0
    chosen = plain_body
    if lax.axis_size("ep") == 4 and gate_weight.shape[0] == 1 and n == LINE and fits:
        chosen = fused_body
    return chosen(tokens, norm_gain, gate_weight, up_weight, down_weight, expert_ids, route_weight)


def solution(mesh):
    placed = (
        P(("grp", "ep", "tp"), None),
        P(),
        P("ep", None, "tp"),
        P("ep", None, "tp"),
        P("ep", "tp", None),
        P(("grp", "ep"), None),
        P(("grp", "ep"), None),
    )
    return jax.shard_map(
        body, mesh=mesh, in_specs=placed, out_specs=P(("grp", "ep", "tp"), None), check_vma=False
    )
```

```python
import functools

import jax
import jax.numpy as jnp
from jax import lax
from jax.experimental import pallas as pl
from jax.experimental.pallas import tpu as pltpu
from jax.sharding import PartitionSpec as P

TOP_K = 2
MESH = pl.DeviceIdType.MESH
VMEM_ROOM = 60 << 20

ACROSS, UP, DOWN = range(3)
RELAY, SEND, REDUCE, COMPUTE = range(4)
UNITS = 2
PIECES = 4
PHASES = 1
LINE = 4
SPREAD = ((1, 15, 15, 5), (8, 13, 15, 1), (13, 11, 14, 7), (8, 7, 13, 14))
GATHER = ((15, 14, 14, 1), (1, 15, 15, 12), (7, 8, 15, 13), (8, 15, 8, 3))
ORDER = (
    (
        (0, 0, 0, 0, 0), (0, 0, 0, 1, 0), (0, 0, 0, 2, 0), (0, 0, 0, 3, 0), (1, 0, 0, 1, 0), (1, 0, 0, 1, 1),
        (1, 0, 0, 0, 0), (1, 0, 0, 3, 1), (3, 0, 0, 0, 0), (1, 0, 0, 2, 0), (1, 0, 0, 2, 1), (3, 0, 0, 1, 0),
        (0, 1, 0, 1, 0), (1, 0, 0, 3, 0), (1, 0, 0, 0, 1), (0, 0, 1, 3, 0), (0, 1, 0, 0, 0), (1, 0, 1, 3, 0),
        (1, 1, 0, 0, 1), (0, 0, 1, 2, 0), (3, 1, 0, 0, 0), (0, 1, 0, 2, 0), (1, 0, 1, 2, 0), (3, 0, 1, 1, 0),
        (0, 1, 0, 3, 0), (0, 0, 1, 0, 0), (2, 1, 0, 0, 0), (2, 1, 0, 1, 1), (0, 0, 1, 1, 0), (1, 1, 0, 3, 1),
        (0, 1, 1, 3, 0), (1, 0, 1, 1, 0), (3, 1, 0, 1, 0), (0, 0, 2, 1, 0), (1, 1, 1, 3, 1), (0, 1, 1, 2, 0),
        (1, 0, 2, 1, 0), (3, 0, 1, 0, 0), (3, 1, 1, 1, 0), (0, 0, 2, 0, 0), (1, 0, 2, 0, 0), (2, 0, 1, 3, 1),
        (0, 0, 3, 3, 0), (0, 1, 1, 1, 0), (1, 1, 1, 1, 1), (3, 0, 2, 0, 0), (0, 0, 3, 2, 0), (0, 1, 2, 1, 0),
        (1, 0, 3, 2, 0), (2, 1, 1, 3, 1), (2, 1, 1, 2, 0), (0, 0, 3, 1, 0), (3, 0, 3, 1, 0), (0, 1, 2, 0, 0),
        (1, 0, 3, 1, 0), (2, 0, 2, 1, 1), (0, 1, 3, 3, 0), (2, 1, 0, 2, 1), (0, 1, 3, 2, 0), (3, 1, 2, 0, 0),
        (0, 0, 2, 3, 0), (2, 0, 3, 2, 1), (1, 0, 2, 3, 0), (3, 1, 3, 1, 0), (0, 1, 2, 2, 0), (2, 1, 2, 1, 1),
        (2, 1, 2, 0, 0), (0, 1, 3, 1, 0), (0, 1, 3, 0, 0), (2, 1, 3, 3, 0), (2, 1, 3, 2, 1), (0, 1, 2, 3, 0),
        (3, 1, 3, 0, 0), (0, 0, 3, 0, 0), (2, 0, 1, 2, 1), (3, 1, 2, 1, 0), (0, 0, 2, 2, 0), (2, 1, 3, 0, 1),
        (2, 1, 3, 1, 0), (3, 0, 3, 0, 0), (0, 1, 1, 0, 0), (2, 1, 2, 2, 0), (2, 0, 3, 3, 1), (3, 0, 2, 1, 0),
        (2, 0, 3, 0, 1), (2, 1, 2, 3, 0), (3, 1, 1, 0, 0), (2, 0, 3, 1, 1), (2, 0, 2, 2, 1), (2, 1, 1, 1, 0),
        (2, 0, 2, 3, 1), (2, 1, 1, 0, 0), (2, 0, 2, 0, 1), (2, 1, 0, 3, 0), (2, 0, 1, 1, 1), (2, 0, 0, 1, 0),
        (2, 0, 1, 0, 1), (2, 0, 0, 0, 0), (2, 0, 0, 3, 0), (2, 0, 0, 2, 0),
    ),
    (
        (0, 0, 1, 0, 0), (0, 0, 1, 3, 0), (0, 0, 1, 1, 0), (0, 0, 1, 2, 0), (1, 0, 1, 3, 2), (1, 0, 1, 0, 1),
        (1, 0, 1, 2, 0), (1, 0, 1, 2, 2), (1, 0, 1, 1, 1), (3, 0, 1, 0, 0), (1, 0, 1, 0, 2), (1, 0, 1, 3, 1),
        (3, 0, 1, 1, 0), (0, 0, 0, 1, 0), (1, 0, 0, 1, 0), (0, 1, 1, 2, 0), (1, 0, 0, 1, 1), (1, 0, 1, 1, 2),
        (0, 0, 2, 1, 0), (0, 0, 0, 3, 0), (1, 0, 2, 1, 0), (1, 0, 2, 1, 2), (1, 0, 0, 3, 1), (0, 0, 2, 0, 0),
        (0, 0, 0, 2, 0), (1, 0, 0, 2, 0), (3, 0, 2, 0, 0), (0, 0, 0, 0, 0), (0, 0, 2, 3, 0), (0, 1, 0, 1, 0),
        (1, 0, 2, 3, 0), (1, 0, 0, 2, 1), (1, 0, 2, 0, 2), (3, 0, 0, 1, 0), (0, 0, 3, 3, 0), (0, 1, 0, 0, 0),
        (0, 1, 2, 1, 0), (1, 1, 0, 0, 1), (1, 0, 3, 3, 0), (1, 0, 3, 3, 2), (3, 0, 0, 0, 0), (0, 0, 3, 2, 0),
        (0, 1, 0, 2, 0), (1, 0, 3, 2, 2), (1, 0, 0, 0, 1), (3, 1, 0, 0, 0), (0, 0, 3, 1, 0), (0, 1, 2, 3, 0),
        (1, 0, 3, 1, 2), (1, 0, 3, 1, 0), (1, 0, 1, 2, 1), (3, 0, 3, 1, 0), (0, 0, 2, 2, 0), (0, 1, 3, 3, 0),
        (0, 1, 0, 3, 0), (1, 0, 2, 2, 0), (1, 1, 3, 3, 2), (1, 1, 2, 1, 1), (2, 1, 0, 0, 0), (0, 1, 3, 0, 0),
        (0, 1, 1, 3, 0), (1, 1, 1, 3, 1), (1, 0, 2, 3, 2), (3, 0, 2, 1, 0), (0, 1, 3, 1, 0), (2, 1, 0, 1, 0),
        (0, 1, 2, 0, 0), (3, 1, 1, 1, 0), (0, 1, 2, 2, 0), (1, 1, 2, 2, 2), (3, 1, 3, 0, 0), (0, 1, 1, 1, 0),
        (0, 1, 3, 2, 0), (2, 1, 1, 2, 0), (1, 1, 3, 0, 2), (3, 1, 2, 0, 0), (0, 0, 3, 0, 0), (1, 0, 3, 0, 2),
        (2, 1, 3, 1, 0), (2, 1, 1, 3, 1), (3, 1, 3, 1, 0), (0, 1, 1, 0, 0), (1, 0, 2, 2, 2), (2, 1, 2, 0, 0),
        (2, 0, 2, 1, 1), (3, 0, 3, 0, 0), (2, 1, 3, 3, 0), (1, 1, 1, 0, 2), (3, 1, 0, 1, 0), (2, 0, 3, 2, 1),
        (3, 1, 2, 1, 0), (2, 1, 2, 1, 1), (2, 1, 0, 2, 0), (3, 1, 1, 0, 0), (2, 1, 2, 3, 1), (2, 1, 2, 2, 0),
        (2, 1, 3, 2, 1), (2, 0, 0, 3, 2), (2, 1, 1, 1, 0), (2, 1, 3, 0, 1), (2, 1, 1, 0, 2), (2, 0, 3, 3, 1),
        (2, 1, 0, 3, 2), (2, 0, 3, 0, 1), (2, 0, 0, 1, 2), (2, 0, 3, 1, 1), (2, 0, 0, 0, 2), (2, 0, 2, 2, 1),
        (2, 0, 0, 2, 2), (2, 0, 2, 3, 1), (2, 0, 2, 0, 1), (2, 0, 1, 2, 0), (2, 0, 1, 1, 0), (2, 0, 1, 3, 0),
        (2, 0, 1, 0, 0),
    ),
    (
        (0, 0, 2, 0, 0), (0, 0, 2, 1, 0), (0, 0, 2, 2, 0), (0, 0, 2, 3, 0), (1, 0, 2, 3, 1), (1, 0, 2, 1, 2),
        (1, 0, 2, 0, 0), (1, 0, 2, 1, 1), (1, 0, 2, 0, 2), (1, 0, 2, 2, 0), (3, 0, 2, 0, 0), (1, 0, 2, 3, 2),
        (1, 0, 2, 2, 1), (1, 0, 2, 3, 0), (3, 0, 2, 1, 0), (0, 0, 1, 0, 0), (0, 0, 3, 3, 0), (0, 1, 2, 0, 0),
        (1, 0, 1, 0, 1), (1, 0, 3, 3, 2), (1, 0, 3, 3, 0), (0, 0, 1, 1, 0), (0, 0, 3, 2, 0), (0, 1, 2, 2, 0),
        (1, 0, 3, 2, 2), (1, 0, 3, 2, 0), (1, 0, 2, 0, 1), (3, 0, 1, 0, 0), (0, 0, 3, 1, 0), (0, 0, 1, 3, 0),
        (0, 1, 2, 3, 0), (1, 0, 1, 1, 0), (1, 0, 3, 1, 2), (1, 0, 1, 1, 1), (3, 0, 3, 1, 0), (0, 0, 0, 1, 0),
        (0, 0, 3, 0, 0), (0, 1, 3, 3, 0), (1, 0, 0, 1, 1), (1, 0, 2, 2, 2), (1, 0, 0, 1, 0), (3, 1, 2, 1, 0),
        (0, 0, 0, 3, 0), (0, 1, 3, 0, 0), (0, 1, 3, 2, 0), (1, 1, 3, 0, 2), (1, 0, 0, 3, 1), (1, 0, 0, 3, 0),
        (3, 0, 3, 0, 0), (0, 0, 0, 2, 0), (0, 1, 1, 1, 0), (1, 0, 0, 2, 1), (1, 0, 0, 2, 0), (1, 1, 2, 0, 2),
        (3, 1, 3, 1, 0), (0, 1, 0, 0, 0), (0, 1, 0, 1, 0), (1, 1, 0, 0, 1), (1, 1, 3, 2, 2), (1, 0, 3, 1, 0),
        (3, 0, 0, 1, 0), (0, 0, 0, 0, 0), (0, 1, 0, 3, 0), (1, 1, 0, 3, 1), (2, 1, 2, 2, 0), (1, 0, 3, 0, 2),
        (3, 1, 0, 0, 0), (0, 0, 1, 2, 0), (0, 1, 0, 2, 0), (1, 0, 1, 2, 1), (1, 0, 1, 2, 0), (3, 0, 0, 0, 0),
        (0, 1, 1, 0, 0), (0, 1, 3, 1, 0), (0, 1, 2, 1, 0), (2, 1, 0, 0, 0), (1, 1, 1, 0, 2), (1, 0, 0, 0, 1),
        (3, 1, 0, 1, 0), (0, 1, 1, 3, 0), (1, 1, 1, 3, 1), (2, 1, 3, 3, 2), (2, 1, 0, 1, 0), (3, 1, 3, 0, 0),
        (0, 1, 1, 2, 0), (1, 1, 2, 3, 1), (2, 1, 0, 2, 0), (3, 0, 1, 1, 0), (2, 0, 1, 0, 2), (1, 0, 1, 3, 1),
        (2, 1, 3, 1, 0), (3, 1, 2, 0, 0), (3, 1, 1, 0, 0), (2, 0, 0, 3, 2), (1, 1, 3, 1, 1), (2, 1, 2, 0, 0),
        (3, 1, 1, 1, 0), (2, 1, 1, 1, 0), (2, 1, 1, 0, 2), (2, 1, 1, 2, 0), (2, 0, 3, 2, 1), (2, 1, 0, 3, 2),
        (2, 1, 1, 3, 0), (2, 1, 2, 1, 1), (2, 0, 0, 1, 2), (2, 1, 2, 3, 0), (2, 0, 0, 0, 2), (2, 1, 3, 2, 1),
        (2, 0, 0, 2, 2), (2, 1, 3, 0, 1), (2, 0, 1, 1, 2), (2, 0, 3, 3, 1), (2, 0, 1, 2, 2), (2, 0, 3, 0, 1),
        (2, 0, 1, 3, 2), (2, 0, 3, 1, 1), (2, 0, 2, 2, 0), (2, 0, 2, 3, 0), (2, 0, 2, 1, 0), (2, 0, 2, 0, 0),
    ),
    (
        (0, 0, 3, 0, 0), (0, 0, 3, 1, 0), (0, 0, 3, 2, 0), (0, 0, 3, 3, 0), (1, 0, 3, 3, 0), (1, 0, 3, 3, 2),
        (1, 0, 3, 0, 0), (1, 0, 3, 2, 2), (3, 0, 3, 0, 0), (1, 0, 3, 1, 2), (1, 0, 3, 2, 0), (3, 0, 3, 1, 0),
        (0, 0, 2, 3, 0), (0, 1, 3, 3, 0), (1, 0, 3, 0, 2), (0, 1, 3, 0, 0), (0, 0, 2, 1, 0), (1, 0, 2, 1, 0),
        (1, 1, 3, 0, 2), (0, 0, 2, 2, 0), (0, 1, 3, 2, 0), (1, 0, 2, 2, 0), (3, 0, 2, 1, 0), (0, 0, 1, 0, 0),
        (0, 1, 2, 1, 0), (1, 0, 1, 0, 0), (3, 1, 3, 1, 0), (0, 0, 2, 0, 0), (0, 1, 2, 2, 0), (1, 0, 2, 0, 0),
        (0, 0, 1, 1, 0), (1, 0, 1, 1, 0), (3, 0, 2, 0, 0), (0, 1, 1, 0, 0), (0, 0, 0, 1, 0), (1, 0, 0, 1, 0),
        (1, 1, 1, 0, 2), (3, 0, 1, 0, 0), (2, 1, 3, 3, 2), (0, 1, 2, 0, 0), (0, 0, 0, 3, 0), (2, 0, 2, 0, 2),
        (3, 1, 2, 0, 0), (0, 0, 0, 2, 0), (0, 1, 1, 1, 0), (2, 0, 1, 0, 2), (1, 0, 0, 2, 0), (0, 1, 0, 1, 0),
        (0, 1, 0, 0, 0), (3, 0, 0, 1, 0), (0, 1, 0, 3, 0), (2, 1, 2, 0, 2), (3, 1, 0, 0, 0), (2, 0, 0, 3, 2),
        (0, 0, 1, 2, 0), (0, 1, 0, 2, 0), (1, 0, 1, 2, 0), (3, 1, 1, 0, 0), (2, 1, 0, 1, 0), (0, 0, 0, 0, 0),
        (3, 1, 0, 1, 0), (2, 1, 1, 0, 2), (2, 1, 0, 0, 0), (3, 0, 0, 0, 0), (0, 1, 1, 2, 0), (0, 1, 1, 3, 0),
        (2, 1, 0, 2, 0), (2, 1, 0, 3, 2), (0, 1, 2, 3, 0), (2, 1, 1, 1, 0), (2, 0, 0, 1, 2), (3, 1, 1, 1, 0),
        (0, 0, 1, 3, 0), (2, 0, 0, 0, 2), (3, 1, 2, 1, 0), (0, 1, 3, 1, 0), (2, 1, 1, 2, 0), (2, 0, 0, 2, 2),
        (3, 0, 1, 1, 0), (2, 1, 1, 3, 0), (3, 1, 3, 0, 0), (2, 1, 2, 3, 0), (2, 0, 1, 1, 2), (2, 0, 1, 2, 2),
        (2, 1, 2, 2, 0), (2, 0, 1, 3, 2), (2, 1, 2, 1, 0), (2, 0, 2, 3, 2), (2, 1, 3, 1, 0), (2, 0, 2, 2, 2),
        (2, 1, 3, 2, 0), (2, 0, 2, 1, 2), (2, 1, 3, 0, 0), (2, 0, 3, 3, 0), (2, 0, 3, 2, 0), (2, 0, 3, 1, 0),
        (2, 0, 3, 0, 0),
    ),
)


def norm_rows(tokens, norm_gain):
    values = tokens.astype(jnp.float32)
    scaled = values * lax.rsqrt(jnp.mean(values * values, axis=-1, keepdims=True) + 1e-06)
    return (scaled * norm_gain).astype(jnp.bfloat16)


def expert_hidden(rows, gate_weight, up_weight):
    gate = jnp.einsum("e...d,edf->e...f", rows, gate_weight, preferred_element_type=jnp.float32)
    upper = jnp.einsum("e...d,edf->e...f", rows, up_weight, preferred_element_type=jnp.float32)
    return (jax.nn.silu(gate) * upper).astype(jnp.bfloat16)


def weigh_pieces(summed, weights):
    piece = lax.optimization_barrier(summed.astype(jnp.bfloat16)).astype(jnp.float32)
    total = piece[:, 0] * weights[:, 0:1]
    total = total + piece[:, 1] * weights[:, 1:2]
    return total.astype(jnp.bfloat16)


def plain_body(tokens, norm_gain, gate_weight, up_weight, down_weight, expert_ids, route_weight):
    tok_rows = tokens.shape[0]
    width = tokens.shape[1]
    local_experts = gate_weight.shape[0]
    inner = gate_weight.shape[2]
    n_tp = lax.axis_size("tp")
    n_ep = lax.axis_size("ep")
    experts = n_ep * local_experts
    most = max(2, tok_rows * TOP_K * 5 // (4 * experts))
    normed = norm_rows(tokens, norm_gain)
    flat_ids = expert_ids.reshape(n_tp, tok_rows * TOP_K)
    onehot = (flat_ids[:, :, None] == jnp.arange(experts, dtype=jnp.int32)[None, None, :]).astype(
        jnp.int32
    )
    before = jnp.cumsum(onehot, axis=1) - onehot
    slots = jnp.sum(before * onehot, axis=-1)
    owner = jnp.arange(n_tp, dtype=jnp.int32)[:, None]
    row_index = (flat_ids * (n_tp * most) + owner * most + slots).reshape(-1)
    mine = lax.axis_index("tp")
    own_ids = lax.dynamic_slice_in_dim(flat_ids, mine, 1, 0)[0]
    own_slots = lax.dynamic_slice_in_dim(slots, mine, 1, 0)[0]
    own_index = own_ids * most + own_slots
    whole = lax.all_gather(normed, "tp", axis=0, tiled=True)
    sending = (
        jnp.zeros((experts * n_tp * most, width), jnp.bfloat16)
        .at[row_index]
        .set(jnp.repeat(whole, TOP_K, axis=0))
    )
    arrived = lax.all_to_all(
        sending.reshape(experts, n_tp * most, width), "ep", split_axis=0, concat_axis=1, tiled=True
    )
    hidden = expert_hidden(arrived, gate_weight, up_weight)
    by_source = hidden.reshape(local_experts, n_ep, n_tp, most, inner).transpose(2, 0, 1, 3, 4)
    per_device = local_experts * n_ep * most
    product = jnp.einsum(
        "tlnmf,lfd->tlnmd", by_source, down_weight, preferred_element_type=jnp.float32
    )
    own_sums = lax.psum_scatter(
        product.astype(jnp.bfloat16)
        .astype(jnp.float32)
        .reshape(per_device * lax.axis_size("tp"), width)
        .astype(jnp.bfloat16),
        "tp",
        scatter_dimension=0,
        tiled=True,
    )
    own_pieces = own_sums.reshape(local_experts, n_ep, most, width)
    back = lax.all_to_all(own_pieces, "ep", split_axis=1, concat_axis=0, tiled=True)
    picked = back.reshape(experts * most, width)[own_index].reshape(tok_rows, TOP_K, width)
    own_weights = lax.dynamic_slice_in_dim(route_weight, mine * tok_rows, tok_rows, 0)
    return weigh_pieces(picked.astype(jnp.float32), own_weights)


def neighbour(n, place, edge, piece):
    row, at, number = piece
    if edge == ACROSS:
        return place, (1 - row, at, number), ACROSS
    there = place + (1 if edge == UP else -1)
    return (there, piece, DOWN if edge == UP else UP) if 0 <= there < n else None


def parent(n, crossings, place, piece):
    row, at, number = piece
    goal = at
    if row:
        bits = crossings[at][number]
        places = [k for k in range(n) if bits >> k & 1]
        goal = min(places, key=lambda k: (abs(k - place), abs(k - at)))
    if goal == place:
        return ACROSS if row else None
    return UP if goal > place else DOWN


def children(n, crossings, place, piece):
    found = []
    for edge in (ACROSS, UP, DOWN):
        there = neighbour(n, place, edge, piece)
        if there is not None and parent(n, crossings, there[0], there[1]) == there[2]:
            found.append(edge)
    return found


def choose(index, low, branches):
    if len(branches) == 1:
        branches[0]()
        return
    half = len(branches) // 2
    lax.cond(
        index < low + half,
        lambda: choose(index, low, branches[:half]),
        lambda: choose(index, low + half, branches[half:]),
    )


def pick(index, values):
    result = values[0]
    for i, value in enumerate(values[1:], 1):
        result = jnp.where(index == i, value, result)
    return result


def split(order):
    before, steps, current = [], [], []
    for op in order:
        if op[0] == COMPUTE:
            before.append(current)
            current = []
            if op[4] == 0:
                steps.append(op[1:4])
        else:
            current.append(op)
    return before, steps, current


def kernel(
    n, tok_hbm, gain_hbm, ids_hbm, weight_hbm, gate_hbm, up_hbm, down_hbm, out_ref,
    tok, gain, ids, weight, both, down, hidden, buf, own_shares, shares, part, srecv, rrecv,
    load_sem, w_s, w_r, sib_s, ag_s, rs_s, ag_r, ags_r, rss_r, rs_r,
):
    ep = lax.axis_index("ep")
    z = lax.axis_index("tp")
    y, c = ep // 2, ep % 2
    rows, width = tok.shape
    inner = down.shape[0]
    experts = shares.shape[0]
    per = PIECES // UNITS
    tall = rows // UNITS
    short = rows // PIECES
    sib = {"ep": 2 * y + 1 - c}
    toward = {ACROSS: {"ep": 2 * (1 - y) + c}, UP: {"tp": z + 1}, DOWN: {"tp": z - 1}}

    def row_of(row):
        return row + (1 - 2 * row) * y

    def first(row, at, unit, lane):
        return (((row * n + at) * UNITS + unit) * 2 + lane) * per

    def remote(src, dst, send, recv, to):
        return pltpu.make_async_remote_copy(
            src_ref=src, dst_ref=dst, send_sem=send, recv_sem=recv, device_id=to, device_id_type=MESH
        )

    barrier = pltpu.get_barrier_semaphore()
    for k in range(1, 4):
        pl.semaphore_signal(barrier, inc=1, device_id={"ep": (ep + k) % 4}, device_id_type=MESH)

    @pl.when(z < n - 1)
    def _():
        pl.semaphore_signal(barrier, inc=1, device_id=toward[UP], device_id_type=MESH)

    @pl.when(z > 0)
    def _():
        pl.semaphore_signal(barrier, inc=1, device_id=toward[DOWN], device_id_type=MESH)

    loads = [
        pltpu.make_async_copy(src, dst, load_sem.at[i])
        for i, (src, dst) in enumerate(
            (
                (tok_hbm, tok),
                (gain_hbm, gain),
                (ids_hbm, ids),
                (weight_hbm, weight),
                (gate_hbm.at[0], both.at[:, pl.ds(0, inner)]),
                (up_hbm.at[0], both.at[:, pl.ds(inner, inner)]),
                (down_hbm.at[0], down),
            )
        )
    ]
    for load in loads:
        load.start()

    loads[0].wait()
    loads[1].wait()
    normed = norm_rows(tok[...], gain[...]).reshape(UNITS, per, short, width)
    for unit in range(UNITS):
        buf[pl.ds(first(y, z, unit, c), per)] = normed[unit]
    loads[2].wait()
    loads[3].wait()
    for e in range(experts):
        named = jnp.where(ids[...] == e, weight[...], 0.0)
        total = named[0:1] + named[1:2]
        for k in range(n):
            own_shares[e, k : k + 1, :] = total[:, k * rows : (k + 1) * rows]

    pl.semaphore_wait(barrier, 3 + jnp.where(z > 0, 1, 0) + jnp.where(z < n - 1, 1, 0))

    def share(k):
        to = (ep + k) % 4
        return remote(own_shares.at[to], shares.at[ep], w_s, w_r, {"ep": to})

    def held(yb, at, number, lane):
        return buf.at[first(yb, at, number // per, lane) + number % per]

    def sum_copy(yb, at, unit):
        return remote(part.at[yb, at, unit, 1 - c], srecv.at[yb, at, unit], sib_s, rss_r.at[yb, at, unit], sib)

    def run(here, ops, waited):
        waited = set(waited)
        for op in ops:
            what, row, at, number, edge = op
            yb = row_of(row)
            unit, piece = number // per, number % per
            mine = held(yb, at, number, c)
            own = row == 0 and at == here
            if what == RELAY:
                if not own:
                    remote(mine, mine, ag_s, ag_r.at[yb, at, number], sib).wait_recv()
                remote(mine, mine, sib_s, ags_r.at[yb, at, unit], sib).start()
            elif what == SEND:
                remote(mine, mine, ag_s, ag_r.at[yb, at, number], toward[edge]).start()
            else:
                if (row, at, unit) not in waited:
                    waited.add((row, at, unit))
                    sum_copy(yb, at, unit).wait_recv()
                total = part[yb, at, unit, c, piece].astype(jnp.float32)
                total = total + srecv[yb, at, unit, piece].astype(jnp.float32)
                count = len(children(n, GATHER, here, (row, at, number)))
                if count:
                    landed = rrecv.at[yb, at, number, pl.ds(0, count)]
                    remote(landed, landed, rs_s, rs_r.at[yb, at, number], sib).wait_recv()
                for slot in range(count):
                    total = total + rrecv[yb, at, number, slot].astype(jnp.float32)
                if own:
                    out_ref[number * short : (number + 1) * short, :] = total.astype(out_ref.dtype)
                else:
                    part[yb, at, unit, c, piece] = total.astype(jnp.bfloat16)
                    there, seen_as, back = neighbour(n, here, edge, (row, at, number))
                    slot = children(n, GATHER, there, seen_as).index(back)
                    remote(
                        part.at[yb, at, unit, c, piece], rrecv.at[yb, at, number, slot],
                        rs_s, rs_r.at[yb, at, number], toward[edge],
                    ).start()

    for k in range(1, 4):
        share(k).start()
    shares[ep] = own_shares[ep]

    plans = [split(order) for order in ORDER]
    steps = len(plans[0][1])
    branches, waited = [[] for _ in range(PHASES)], [set() for _ in plans]
    for here, (before, _, _) in enumerate(plans):
        for slot, ops in enumerate(before):
            branches[slot % PHASES].append(functools.partial(run, here, ops, waited[here]))
            waited[here] = waited[here] | {(op[1], op[2], op[3] // per) for op in ops if op[0] == REDUCE}

    def column(row):
        return jnp.transpose(jnp.broadcast_to(row, (rows, rows)))[:, :1]

    lane = lax.broadcasted_iota(jnp.int32, (8, rows), 1)

    def one(step, carry):
        choose(z * steps + step, 0, branches[0])

        @pl.when(step == 0)
        def _():
            for load in loads[4:]:
                load.wait()

        code = pick(z, [pick(step, [(s[0] * n + s[1]) * UNITS + s[2] for s in plan[1]]) for plan in plans])
        row, at, unit = code // (n * UNITS), code // UNITS % n, code % UNITS
        yb = row_of(row)
        theirs = buf.at[pl.ds(first(yb, at, unit, 1 - c), per)]
        remote(theirs, theirs, sib_s, ags_r.at[yb, at, unit], sib).wait_recv()
        x = buf[pl.ds(first(yb, at, unit, 0), 2 * per)].reshape(2 * tall, width)
        mixed = jnp.dot(x, both[...], preferred_element_type=jnp.float32)
        hidden[...] = (jax.nn.silu(mixed[:, :inner]) * mixed[:, inner:]).astype(jnp.bfloat16)
        for later in branches[1:]:
            choose(z * steps + step, 0, later)
        product = jnp.dot(hidden[...], down[...], preferred_element_type=jnp.float32)

        @pl.when(step == 0)
        def _():
            remote(own_shares.at[pl.ds(0, 3)], shares.at[pl.ds(0, 3)], w_s, w_r, sib).wait_recv()

        ours = [jnp.broadcast_to(shares[2 * yb + half, pl.ds(at, 1), :], (8, rows)) for half in range(2)]
        turned = [pltpu.roll(values, tall, 1) for values in ours]
        early = jnp.where(lane < tall, ours[0], turned[1])
        late = jnp.where(lane < tall, turned[0], ours[1])
        w = column(jnp.where(unit == 0, early, late)[0:1])
        part[yb, at, unit] = (product * w).astype(jnp.bfloat16).reshape(2, per, short, width)
        sum_copy(yb, at, unit).start()
        return carry

    lax.fori_loop(0, steps, one, 0)

    def finish(here):
        run(here, plans[here][2], waited[here])
        for what, sem in ((SEND, ag_s), (REDUCE, rs_s)):
            count = sum(op[0] == what and (what == SEND or op[1] > 0 or op[2] != here) for op in ORDER[here])
            sent = buf.at[pl.ds(0, count)]
            remote(sent, sent, sem, sem, sib).wait_send()

    choose(z, 0, [functools.partial(finish, here) for here in range(len(plans))])
    remote(buf, buf, sib_s, sib_s, sib).wait_send()
    remote(own_shares.at[pl.ds(0, 3)], shares.at[pl.ds(0, 3)], w_s, w_r, sib).wait_send()


def kernel_bytes(n, rows, width, inner):
    blocks = n * 4 + 2 * n * 2 + 2 * n + 6 * n + 4
    return 2 * width * (3 * inner + blocks * rows) + 16 * rows * (width + 2 * inner)


def fused_body(tokens, norm_gain, gate_weight, up_weight, down_weight, expert_ids, route_weight):
    rows, width = tokens.shape
    inner = gate_weight.shape[2]
    n = lax.axis_size("tp")
    experts = lax.axis_size("ep")
    vmem = pl.BlockSpec(memory_space=pltpu.VMEM)
    anywhere = pl.BlockSpec(memory_space=pl.ANY)
    dma = pltpu.SemaphoreType.DMA
    bf16 = jnp.bfloat16
    per, short = PIECES // UNITS, rows // PIECES
    return pl.pallas_call(
        functools.partial(kernel, n),
        out_shape=jax.ShapeDtypeStruct((rows, width), bf16),
        in_specs=[anywhere] * 7,
        out_specs=vmem,
        scratch_shapes=[
            pltpu.VMEM((rows, width), bf16),
            pltpu.VMEM((1, width), jnp.float32),
            pltpu.VMEM((TOP_K, n * rows), jnp.int32),
            pltpu.VMEM((TOP_K, n * rows), jnp.float32),
            pltpu.VMEM((width, 2 * inner), bf16),
            pltpu.VMEM((inner, width), bf16),
            pltpu.VMEM((2 * rows // UNITS, inner), bf16),
            pltpu.VMEM((2 * n * UNITS * 2 * per, short, width), bf16),
            pltpu.VMEM((experts, n, rows), jnp.float32),
            pltpu.VMEM((experts, n, rows), jnp.float32),
            pltpu.VMEM((2, n, UNITS, 2, per, short, width), bf16),
            pltpu.VMEM((2, n, UNITS, per, short, width), bf16),
            pltpu.VMEM((2, n, PIECES, 3, short, width), bf16),
            dma((7,)),
            dma,
            dma,
            dma,
            dma,
            dma,
            dma((2, n, PIECES)),
            dma((2, n, UNITS)),
            dma((2, n, UNITS)),
            dma((2, n, PIECES)),
        ],
        compiler_params=pltpu.CompilerParams(
            collective_id=0, has_side_effects=True, vmem_limit_bytes=VMEM_ROOM
        ),
    )(tokens, norm_gain.reshape(1, width), expert_ids.T, route_weight.T, gate_weight, up_weight, down_weight)


def body(tokens, norm_gain, gate_weight, up_weight, down_weight, expert_ids, route_weight):
    rows, width = tokens.shape
    inner = gate_weight.shape[2]
    n = lax.axis_size("tp")
    fits = kernel_bytes(n, rows, width, inner) <= VMEM_ROOM and rows % 128 == 0
    chosen = plain_body
    if lax.axis_size("ep") == 4 and gate_weight.shape[0] == 1 and n == LINE and fits:
        chosen = fused_body
    return chosen(tokens, norm_gain, gate_weight, up_weight, down_weight, expert_ids, route_weight)


def solution(mesh):
    placed = (
        P(("grp", "ep", "tp"), None),
        P(),
        P("ep", None, "tp"),
        P("ep", None, "tp"),
        P("ep", "tp", None),
        P(("grp", "ep"), None),
        P(("grp", "ep"), None),
    )
    return jax.shard_map(
        body, mesh=mesh, in_specs=placed, out_specs=P(("grp", "ep", "tp"), None), check_vma=False
    )
```
